128 devices in a mesh: tp: 16 (over z, y), dp: 8 (over x, core).
Axes of the slice: x: 4, y: 4, z: 4, core: 2. Of those that a mesh axis runs over, the one named last changes fastest.
Arguments:
- tokens: bfloat16 [256, 4096], P('tp', 'dp'), may hold values from -10 to 10
- norm_gain: float32 [2, 4096], P(None, 'dp'), may hold values from 0.1 to 1.9
- input_weight: bfloat16 [2, 4096, 1024], P(None, 'dp', 'tp'), may hold values from -0.09375 to 0.09375
- decay_rate: float32 [2, 64, 64], P(None, 'tp'), may hold values from 0.01 to 1
- frequency: float32 [2, 64, 64], P(None, 'tp'), may hold values from 0.5 to 3
- step_size: float32 [2, 64], P(None, 'tp'), may hold values from 0.1 to 1
- state_in: float32 [2, 64, 16, 128], P(None, 'tp'), may hold values from -1.5 to 1.5
- readout: float32 [2, 64, 16, 128], P(None, 'tp'), may hold values from -0.5 to 0.5
- skip_gain: float32 [2, 1024], P(None, 'tp'), may hold values from -3 to 3
- value_weight: bfloat16 [2, 1024, 4096], P(None, 'tp', 'dp'), may hold values from -0.1875 to 0.1875
- gate_weight: bfloat16 [2, 1024, 4096], P(None, 'tp', 'dp'), may hold values from -0.1875 to 0.1875
- states: float32 [2, 256, 64, 128], P(None, 'dp', 'tp'), may hold values from -3 to 3
Outputs:
- tokens_out: bfloat16 [256, 4096], P('tp', 'dp')
- states_out: float32 [2, 256, 64, 128], P(None, 'dp', 'tp')
The draws below stay inside these ranges and needn't reach their ends.
All inputs are finite; a program needn't handle non-finite values.
Results may differ from the reference program's by a relative error of at most 0.007.
Values may be sent and summed in bfloat16 or wider, within the bound.
A program may use at most 64 MiB of HBM per device.

```python
import math
import jax
import jax.numpy as jnp
from jax import lax

D = 4096
S = 1024
GS = 16
P_SIZE = 64
LAYERS = 2
G = 64
BATCH = 256


def draw_tokens(key, part):
    first, second, third = jax.random.split(key, 3)
    column_scale = jnp.exp(jax.random.uniform(second, (32,), jnp.float32, -0.7, 0.7))
    column_scale = jnp.repeat(column_scale, D // 32)
    base = jnp.clip(jax.random.normal(first, (BATCH, D), jnp.float32), -4.0, 4.0)
    return (base * column_scale[None, :]).astype(jnp.bfloat16)


def steps_of(stream_key, dims, pieces, smallest, top_value):
    def one(position, blocks):
        steps = jax.random.uniform(jax.random.fold_in(jax.random.fold_in(stream_key, 6), position), (blocks,), jnp.float32, smallest / len(pieces), top_value / len(pieces))
        return jnp.repeat(jnp.exp(steps), dims[position] // blocks).reshape((-1,) + (1,) * (len(dims) - position - 1))

    level = one(*pieces[0])
    for cut in pieces[1:]:
        level = level * one(*cut)
    return level


def bell_draw(stream_key, dims, spread, most, pieces=(), dtype=jnp.bfloat16):
    result = jax.random.normal(stream_key, dims, jnp.float32) * spread
    if len(pieces) > 0:
        result = steps_of(stream_key, dims, pieces, -0.22, 0.18) * result
    return jnp.clip(result, min=-most, max=most).astype(dtype)


def setup_inputs(seed: int = 0) -> dict:
    seeds = jax.random.split(jax.random.key(seed), 13)
    tokens = draw_tokens(jax.random.fold_in(seeds[12], 71), 0)
    norm_gain = jnp.clip(1.0 + 0.18 * jax.random.normal(seeds[1], (LAYERS, D), jnp.float32), 0.1, 1.9)
    input_weight = bell_draw(seeds[2], (LAYERS, D, S), D ** -0.5, 0.09375, ((1, 8), (2, 16)))
    decay_rate = jnp.clip(jnp.exp(math.log(1.0) - 4.6051702 * jax.random.uniform(seeds[3], (LAYERS, G, P_SIZE), jnp.float32) ** steps_of(seeds[3], (LAYERS, G, P_SIZE), ((1, 16),), -0.2, 0.2)), 0.01, 1.0)
    frequency = jnp.clip(0.5 + 2.5 * jax.random.uniform(seeds[4], (LAYERS, G, P_SIZE), jnp.float32) ** steps_of(seeds[4], (LAYERS, G, P_SIZE), ((1, 16),), -0.2, 0.2), 0.5, 3.0)
    step_size = jnp.clip(jnp.exp(math.log(1.0) - 2.3025851 * jax.random.uniform(seeds[5], (LAYERS, G), jnp.float32) ** steps_of(seeds[5], (LAYERS, G), ((1, 16),), -0.2, 0.2)), 0.1, 1.0)
    state_in = bell_draw(seeds[6], (LAYERS, G, GS, 2 * P_SIZE), GS ** -0.5, 1.5, ((1, 16),), jnp.float32)
    readout = bell_draw(seeds[7], (LAYERS, G, GS, 2 * P_SIZE), (2 * P_SIZE) ** -0.5, 0.5, ((1, 16),), jnp.float32)
    skip_gain = bell_draw(seeds[8], (LAYERS, S), 0.5, 3.0, ((1, 16),), jnp.float32)
    value_weight = bell_draw(seeds[9], (LAYERS, S, D), S ** -0.5, 0.1875, ((1, 16), (2, 8)))
    gate_weight = bell_draw(seeds[10], (LAYERS, S, D), S ** -0.5, 0.1875, ((1, 16), (2, 8)))
    states = bell_draw(seeds[11], (LAYERS, BATCH, G, 2 * P_SIZE), 0.5, 3.0, ((1, 8), (2, 16)), jnp.float32)
    return dict(tokens=tokens, norm_gain=norm_gain, input_weight=input_weight, decay_rate=decay_rate, frequency=frequency, step_size=step_size, state_in=state_in, readout=readout, skip_gain=skip_gain, value_weight=value_weight, gate_weight=gate_weight, states=states)


epsilon = 1e-06

def transition(rate, frequency, step):
    magnitude = jnp.exp(-rate * step[:, None])
    angle = frequency * step[:, None]
    keep_real = magnitude * jnp.cos(angle)
    keep_imag = magnitude * jnp.sin(angle)
    minus_one = keep_real - 1.0
    denominator = rate * rate + frequency * frequency
    lift_real = (-minus_one * rate + keep_imag * frequency) / denominator
    lift_imag = (-keep_imag * rate - minus_one * frequency) / denominator
    return (keep_real, keep_imag, lift_real, lift_imag)

def update(drive, state, rate, frequency, step, state_in, readout, skip):
    groups = rate.shape[0]
    half = state.shape[-1] // 2
    grouped = drive.reshape(drive.shape[0], groups, -1)
    pushed = jnp.einsum('sgc,gcq->sgq', grouped, state_in, precision=lax.Precision.HIGHEST)
    keep_real, keep_imag, lift_real, lift_imag = transition(rate, frequency, step)
    push_real, push_imag = (pushed[..., :half], pushed[..., half:])
    old_real, old_imag = (state[..., :half], state[..., half:])
    new_real = keep_real * old_real - keep_imag * old_imag + lift_real * push_real - lift_imag * push_imag
    new_imag = keep_real * old_imag + keep_imag * old_real + lift_real * push_imag + lift_imag * push_real
    new_state = jnp.concatenate([new_real, new_imag], axis=-1)
    summed = jnp.einsum('sgq,gcq->sgc', new_state, readout, precision=lax.Precision.HIGHEST)
    value = summed.reshape(drive.shape) + skip[None, :] * drive
    return (new_state, jax.nn.gelu(value).astype(jnp.bfloat16))

def reference(tokens, norm_gain, input_weight, decay_rate, frequency, step_size, state_in, readout, skip_gain, value_weight, gate_weight, states):
    current = tokens
    updated = []
    for depth_index in range(LAYERS):
        widened = current.astype(jnp.float32)
        mean_square = lax.optimization_barrier(jnp.mean(widened * widened, axis=1))
        gained = (widened * norm_gain[depth_index][None, :]).astype(jnp.bfloat16)
        drive = jnp.dot(gained, input_weight[depth_index], preferred_element_type=jnp.float32)
        drive = drive * lax.rsqrt(mean_square + epsilon)[:, None]
        new_state, readout_value = update(drive, states[depth_index], decay_rate[depth_index], frequency[depth_index], step_size[depth_index], state_in[depth_index], readout[depth_index], skip_gain[depth_index])
        updated.append(new_state)
        value = jnp.dot(readout_value, value_weight[depth_index], preferred_element_type=jnp.float32)
        gate = jnp.dot(readout_value, gate_weight[depth_index], preferred_element_type=jnp.float32)
        current = (widened + value * jax.nn.sigmoid(gate)).astype(jnp.bfloat16)
    return (current, jnp.stack(updated))
```

```python
import jax
import jax.numpy as jnp
from jax import lax
from jax.experimental import pallas as pl
from jax.experimental.pallas import tpu as pltpu
from jax.sharding import PartitionSpec as P

D = 4096
L = 2
EPS = 1e-06
MESH = pl.DeviceIdType.MESH
F32 = jnp.float32
BF16 = jnp.bfloat16
HIGH = lax.Precision.HIGHEST


def nt(a, b, precision=None):
    return lax.dot_general(
        a, b, (((1,), (1,)), ((), ())), precision=precision, preferred_element_type=F32
    )


def device(z, y, x, c):
    return (z * 4 + y, x * 2 + c)


class Sends:
    def __init__(self):
        self.waits = []

    def go(self, src, dst, send_sem, recv_sem, to, here=None):
        copy = pltpu.make_async_remote_copy(
            src_ref=src, dst_ref=dst, send_sem=send_sem, recv_sem=recv_sem,
            device_id=to, device_id_type=MESH,
        )
        if here is None:
            copy.start()
            self.waits.append((None, copy))
            return

        @pl.when(here)
        def _():
            pltpu.make_async_copy(src, dst, recv_sem).start()

        @pl.when(jnp.logical_not(here))
        def _():
            copy.start()

        self.waits.append((jnp.logical_not(here), copy))

    def finish(self):
        for away, copy in self.waits:
            if away is None:
                copy.wait_send()
            else:
                @pl.when(away)
                def _(copy=copy):
                    copy.wait_send()


def arrived(dst, sem):
    pltpu.make_async_copy(dst, dst, sem).wait()


def kernel(
    tok, gain, win, decay, freq, step, sin, rdo, skip, wv, wg, st,
    tok_out, st_out,
    xg, wi, wo, gain_v, decay_v, freq_v, step_v, sin_v, rdo_v, skip_v, st_v,
    big_b, m3, base, ks, pb, sq, bm, bq, cs, cr, part, rs, rr, new_v, out_v,
    load, load_w, load_o, load_st, a_s, a_r, w_s, w_r, o_s, o_r,
    b_s, b_r, q_s, q_r, c_s, c_r, r_s, r_r, done,
):
    t, d = lax.axis_index("tp"), lax.axis_index("dp")
    z, y, x, c = t // 4, t % 4, d // 2, d % 2
    barrier = pltpu.get_barrier_semaphore()
    greeted = [(z, (y + i) % 4, x, c) for i in (1, 2, 3)]
    greeted += [((z + i) % 4, y, x, c) for i in (1, 2, 3)]
    greeted += [(z, y, (x + i) % 4, (c + k) % 2) for i in range(4) for k in range(2) if i + k]
    for peer in greeted:
        pl.semaphore_signal(barrier, inc=1, device_id=device(*peer), device_id_type=MESH)

    loads = [
        pltpu.make_async_copy(tok, xg.at[0, y], a_r.at[0, y]),
        pltpu.make_async_copy(win.at[0], wi.at[0, 0], load_w.at[0]),
    ]
    small = [(decay, decay_v), (freq, freq_v), (step, step_v), (sin, sin_v), (rdo, rdo_v),
             (skip, skip_v), (gain, gain_v)]
    small_loads = [
        pltpu.make_async_copy(src, dst, load.at[i]) for i, (src, dst) in enumerate(small)
    ]
    st_load = pltpu.make_async_copy(st, st_v, load_st.at[0])
    wo_loads = []
    for l in range(L):
        for k, w in enumerate((wv, wg)):
            wo_loads.append(pltpu.make_async_copy(w.at[l], wo.at[l, y, k], load_o.at[l, k]))
    w1_load = pltpu.make_async_copy(win.at[1], wi.at[1, 0], load_w.at[1])
    for copy in loads + wo_loads[:2] + small_loads + [st_load, w1_load] + wo_loads[2:]:
        copy.start()

    sends = Sends()

    loads[1].wait()
    loads[0].wait()
    pl.semaphore_wait(barrier, len(greeted))

    def send_x(l):
        for i in (1, 3, 2):
            sends.go(xg.at[l, y], xg.at[l, y], a_s.at[l, i], a_r.at[l, y],
                     device(z, (y + i) % 4, x, c))

    def send_win(l):
        for i in (2, 1, 3):
            sends.go(wi.at[l, 0], wi.at[l, i], w_s.at[l, i], w_r.at[l, i],
                     device((z + i) % 4, y, x, c))

    def send_wo(l):
        for i in (1, 3, 2):
            sends.go(wo.at[l, y], wo.at[l, y], o_s.at[l, i], o_r.at[l, y],
                     device(z, (y + i) % 4, x, c))

    send_x(0)
    send_win(0)
    wo_loads[0].wait()
    wo_loads[1].wait()
    send_wo(0)

    for copy in small_loads:
        copy.wait()
    rate = jnp.concatenate([decay_v[0], decay_v[1]], axis=0)
    often = jnp.concatenate([freq_v[0], freq_v[1]], axis=0)
    steps = step_v[...]
    times = jnp.concatenate(
        [jnp.broadcast_to(steps[l:l + 1, g:g + 1], (1, 64)) for l in range(L) for g in range(4)],
        axis=0,
    )
    magnitude = jnp.exp(-rate * times)
    angle = often * times
    keep_r = magnitude * jnp.cos(angle)
    keep_i = magnitude * jnp.sin(angle)
    minus = keep_r - 1.0
    below = rate * rate + often * often
    lift_r = (-minus * rate + keep_i * often) / below
    lift_i = (-keep_i * rate - minus * often) / below
    keep_r = jnp.concatenate([keep_r, keep_r], axis=1)
    keep_i = jnp.concatenate([-keep_i, keep_i], axis=1)
    lift_r = jnp.concatenate([lift_r, lift_r], axis=1)
    lift_i = jnp.concatenate([-lift_i, lift_i], axis=1)

    rows = lax.broadcasted_iota(jnp.int32, (128, 128), 0)
    lanes = lax.broadcasted_iota(jnp.int32, (128, 128), 1)
    same_group = rows // 16 == lanes // 16
    lane16 = lax.broadcasted_iota(jnp.int32, (16, 128), 1)
    row16 = lax.broadcasted_iota(jnp.int32, (16, 128), 0)
    low = lane16 < 64

    st_load.wait()
    for l in range(L):
        lifted = []
        for g in range(4):
            k = l * 4 + g
            b = sin_v[l, g]
            lifted.append(lift_r[k:k + 1] * b + lift_i[k:k + 1] * pltpu.roll(b, 64, 1))
        both = jnp.concatenate(lifted + lifted, axis=0)
        big_b[l] = both
        out = jnp.concatenate([rdo_v[l, g] for g in range(4)] * 2, axis=0)
        skips = jnp.concatenate([skip_v[l:l + 1], skip_v[l:l + 1]], axis=1)
        m = jnp.where(same_group, nt(both, out, HIGH), 0.0)
        m = m + jnp.where(rows == lanes, jnp.broadcast_to(skips, (128, 128)), 0.0)
        hi = m.astype(BF16)
        m3[l] = jnp.concatenate([hi, hi, (m - hi.astype(F32)).astype(BF16)], axis=0)
        for g in range(4):
            k = l * 4 + g
            s = st_v[l, :, g, :]
            kept = keep_r[k:k + 1] * s + keep_i[k:k + 1] * pltpu.roll(s, 64, 1)
            ks[l, g * 2] = kept[:16]
            ks[l, g * 2 + 1] = kept[16:]
        prod = nt(ks[l].reshape(128, 128), out, HIGH)
        total = jnp.zeros((16, 128), F32)
        for g in range(4):
            for h in range(2):
                block = prod[(g * 2 + h) * 16:(g * 2 + h) * 16 + 16]
                total = total + jnp.where(lane16 // 16 == h * 4 + g, block, 0.0)
        base[l] = total

    w1_load.wait()

    for l in range(L):
        for k in range(4):
            @pl.when(y != k)
            def _(k=k):
                arrived(xg.at[l, k], a_r.at[l, k])
        wide = xg[l].reshape(64, 512).astype(F32)
        gained = (wide * gain_v[l:l + 1]).astype(BF16)
        square = jnp.sum(wide * wide, axis=1, keepdims=True)
        row32 = lax.broadcasted_iota(jnp.int32, (32, 128), 0)
        lane32 = lax.broadcasted_iota(jnp.int32, (32, 128), 1)
        for k in range(2):
            part_sq = jnp.where(row32 == lane32, square[k * 32:k * 32 + 32], 0.0)
            sq[l, k] = jnp.broadcast_to(jnp.sum(part_sq, axis=0, keepdims=True), (8, 128))
        for i in (0, 1, 3, 2):
            if i:
                arrived(wi.at[l, i], w_r.at[l, i])
            twice = jnp.concatenate([wi[l, i], wi[l, i]], axis=0)
            prod = nt(gained, twice)
            zz = (z - i) % 4
            for k in range(2):
                a = prod[k * 32:k * 32 + 16]
                b = prod[k * 32 + 16:k * 32 + 32]
                pb[l, i, k] = jnp.where(low, a, b).astype(BF16)
            for k in range(2):
                to = device(zz, y, z, k)
                here = None if i else jnp.logical_and(x == z, c == k)
                slot = x * 2 + c
                sends.go(pb.at[l, i, k], bm.at[l, slot], b_s.at[l, i * 2 + k], b_r.at[l, slot],
                         to, here)
                sends.go(sq.at[l, k], bq.at[l, slot], q_s.at[l, i * 2 + k], q_r.at[l, slot],
                         to, here)
        if l == 0:
            send_win(1)

        for k in range(8):
            arrived(bq.at[l, k], q_r.at[l, k])
            arrived(bm.at[l, k], b_r.at[l, k])
        squares = bq[l, 0]
        raw = bm[l, 0].astype(F32)
        for k in range(1, 8):
            squares = squares + bq[l, k]
            raw = raw + bm[l, k].astype(F32)
        hi = raw.astype(BF16)
        lo = (raw - hi.astype(F32)).astype(BF16)
        mixed = jnp.dot(
            jnp.concatenate([hi, lo, hi], axis=1), m3[l], preferred_element_type=F32
        )
        spread = jnp.broadcast_to(squares[0:1], (16, 128))
        first = jnp.sum(jnp.where(lane16 == row16, spread, 0.0), axis=1, keepdims=True)
        second = jnp.sum(jnp.where(lane16 == row16 + 16, spread, 0.0), axis=1, keepdims=True)
        scale = lax.rsqrt(jnp.where(low, first, second) * (1.0 / D) + EPS)
        ready = jax.nn.gelu(base[l] + scale * mixed)
        turned = pltpu.roll(ready, 64, 1)
        side = y % 2
        for h in range(2):
            placed = jnp.where(side == h, ready, turned)
            cs[l, h] = jnp.where(lane16 // 64 == side, placed, 0.0).astype(BF16)
        for h in range(2):
            yy = 2 * c + h
            for i in (2, 1, 3, 0):
                for k in range(2):
                    here = y == yy if i + k == 0 else None
                    sends.go(cs.at[l, h], cr.at[l, x, y], c_s.at[l, h * 8 + i * 2 + k],
                             c_r.at[l, x, y], device(z, yy, (x + i) % 4, (c + k) % 2), here)
        if l == 0:
            wo_loads[2].wait()
            wo_loads[3].wait()
            send_wo(1)

        drive = scale * raw
        pieces = [
            jnp.where(lane16 // 16 == h * 4 + g, drive, 0.0) for g in range(4) for h in range(2)
        ]
        push = jnp.dot(
            jnp.concatenate(pieces, axis=0), big_b[l], precision=HIGH, preferred_element_type=F32
        )
        for g in range(4):
            for h in range(2):
                k = g * 2 + h
                new_v[l, h * 16:h * 16 + 16, g, :] = ks[l, k] + push[k * 16:k * 16 + 16]
        pltpu.make_async_copy(new_v.at[l], st_out.at[l], done.at[l]).start()

        for k in range(4):
            @pl.when(y != k)
            def _(k=k):
                arrived(wo.at[l, k], o_r.at[l, k])
        for i in range(4):
            for k in range(4):
                arrived(cr.at[l, i, k], c_r.at[l, i, k])
        left = jnp.concatenate(
            [
                (cr[l, :, 2 * j] + cr[l, :, 2 * j + 1]).reshape(64, 128)
                for j in range(2)
            ],
            axis=1,
        )
        for k in range(2):
            prod = jnp.dot(left, wo[l, :, k].reshape(256, 512), preferred_element_type=F32)
            for i in range(4):
                part[l, i, k] = prod[i * 16:i * 16 + 16]
                rs[l, i, k] = prod[i * 16:i * 16 + 16].astype(BF16)
        for i in (2, 1, 3):
            zz = (z + i) % 4
            sends.go(rs.at[l, zz], rr.at[l, i], r_s.at[l, i], r_r.at[l, i], device(zz, y, x, c))
        value, gate = part[l, z, 0], part[l, z, 1]
        for i in (1, 3, 2):
            arrived(rr.at[l, i], r_r.at[l, i])
            value = value + rr[l, i, 0].astype(F32)
            gate = gate + rr[l, i, 1].astype(F32)
        current = (xg[l, y].astype(F32) + value * jax.nn.sigmoid(gate)).astype(BF16)
        if l + 1 < L:
            xg[l + 1, y] = current
            send_x(l + 1)
        else:
            out_v[...] = current
            copy = pltpu.make_async_copy(out_v, tok_out, done.at[L])
            copy.start()
            copy.wait()
    sends.finish()
    for l in range(L):
        pltpu.make_async_copy(new_v.at[l], st_out.at[l], done.at[l]).wait()


def body(*args):
    args = list(args)
    args[2] = jnp.swapaxes(args[2], 1, 2)
    dma = pltpu.SemaphoreType.DMA
    v = pltpu.VMEM
    anywhere = pl.BlockSpec(memory_space=pl.ANY)
    scratch = [
        v((L, 4, 16, 512), BF16),
        v((L, 4, 64, 512), BF16),
        v((L, 4, 2, 64, 512), BF16),
        v((L, 512), F32),
        v((L, 4, 64), F32),
        v((L, 4, 64), F32),
        v((L, 4), F32),
        v((L, 4, 16, 128), F32),
        v((L, 4, 16, 128), F32),
        v((L, 64), F32),
        v((L, 32, 4, 128), F32),
        v((L, 128, 128), F32),
        v((L, 384, 128), BF16),
        v((L, 16, 128), F32),
        v((L, 8, 16, 128), F32),
        v((L, 4, 2, 16, 128), BF16),
        v((L, 2, 8, 128), F32),
        v((L, 8, 16, 128), BF16),
        v((L, 8, 8, 128), F32),
        v((L, 2, 16, 128), BF16),
        v((L, 4, 4, 16, 128), BF16),
        v((L, 4, 2, 16, 512), F32),
        v((L, 4, 2, 16, 512), BF16),
        v((L, 4, 2, 16, 512), BF16),
        v((L, 32, 4, 128), F32),
        v((16, 512), BF16),
        dma((7,)), dma((L,)), dma((L, 2)), dma((1,)),
        dma((L, 4)), dma((L, 4)),
        dma((L, 4)), dma((L, 4)),
        dma((L, 4)), dma((L, 4)),
        dma((L, 8)), dma((L, 8)),
        dma((L, 8)), dma((L, 8)),
        dma((L, 16)), dma((L, 4, 4)),
        dma((L, 4)), dma((L, 4)),
        dma((L + 1,)),
    ]
    return pl.pallas_call(
        kernel,
        out_shape=(
            jax.ShapeDtypeStruct((16, 512), BF16),
            jax.ShapeDtypeStruct((L, 32, 4, 128), F32),
        ),
        in_specs=[anywhere] * 12,
        out_specs=(anywhere, anywhere),
        scratch_shapes=scratch,
        compiler_params=pltpu.CompilerParams(collective_id=0, has_side_effects=True),
        name="layers",
    )(*args)


def solution(mesh):
    in_specs = (
        P("tp", "dp"),
        P(None, "dp"),
        P(None, "dp", "tp"),
        P(None, "tp", None),
        P(None, "tp", None),
        P(None, "tp"),
        P(None, "tp", None, None),
        P(None, "tp", None, None),
        P(None, "tp"),
        P(None, "tp", "dp"),
        P(None, "tp", "dp"),
        P(None, "dp", "tp", None),
    )
    out_specs = (P("tp", "dp"), P(None, "dp", "tp", None))
    return jax.shard_map(body, mesh=mesh, in_specs=in_specs, out_specs=out_specs, check_vma=False)
```

```python
import jax
import jax.numpy as jnp
from jax import lax
from jax.experimental import pallas as pl
from jax.experimental.pallas import tpu as pltpu
from jax.sharding import PartitionSpec as P

D = 4096
L = 2
EPS = 1e-06
MESH = pl.DeviceIdType.MESH
F32 = jnp.float32
BF16 = jnp.bfloat16
HIGH = lax.Precision.HIGHEST


def nt(a, b, precision=None):
    return lax.dot_general(
        a, b, (((1,), (1,)), ((), ())), precision=precision, preferred_element_type=F32
    )


def device(z, y, x, c):
    return (z * 4 + y, x * 2 + c)


class Sends:
    def __init__(self):
        self.waits = []

    def go(self, src, dst, send_sem, recv_sem, to, here=None):
        copy = pltpu.make_async_remote_copy(
            src_ref=src, dst_ref=dst, send_sem=send_sem, recv_sem=recv_sem,
            device_id=to, device_id_type=MESH,
        )
        if here is None:
            copy.start()
            self.waits.append((None, copy))
            return

        @pl.when(here)
        def _():
            pltpu.make_async_copy(src, dst, recv_sem).start()

        @pl.when(jnp.logical_not(here))
        def _():
            copy.start()

        self.waits.append((jnp.logical_not(here), copy))

    def finish(self):
        for away, copy in self.waits:
            if away is None:
                copy.wait_send()
            else:
                @pl.when(away)
                def _(copy=copy):
                    copy.wait_send()


def arrived(dst, sem):
    pltpu.make_async_copy(dst, dst, sem).wait()


def kernel(
    tok, gain, win, decay, freq, step, sin, rdo, skip, wv, wg, st,
    tok_out, st_out,
    xg, wi, wt, w_raw, w0, wo, gain_v, gain_all, decay_v, freq_v, step_v, sin_v, rdo_v, skip_v, st_v,
    big_b, m3, base, ks, pb, sq, bm, bq, rg, res0, xa, res1, cs, cr, part, rs, rr, new_v, out_v,
    load, load_st, load_w, load_o, load_x, a_s, a_r, w_s, w_r, o_s, o_r,
    b_s, b_r, q_s, q_r, c_s, c_r, r_s, r_r, t_s, t_r, tf_s, g_s, g_r, h_s, h_r, hf_s,
    k_s, k_r, n_s, n_r, e_s, e_r, near_sem, far_sem, done,
):
    t, d = lax.axis_index("tp"), lax.axis_index("dp")
    z, y, x, c = t // 4, t % 4, d // 2, d % 2
    other = 1 - c
    barrier = pltpu.get_barrier_semaphore()
    greeted = [(z, (y + i) % 4, x, c) for i in (1, 2, 3)]
    greeted += [((z + i) % 4, y, x, c) for i in (1, 2, 3)]
    greeted += [(z, y, (x + i) % 4, (c + k) % 2) for i in range(4) for k in range(2) if i + k]
    for peer in greeted:
        pl.semaphore_signal(barrier, inc=1, device_id=device(*peer), device_id_type=MESH)

    tok_load = pltpu.make_async_copy(tok, xg.at[y], load_x.at[0])
    win_loads = [
        pltpu.make_async_copy(win.at[0], wi.at[0], load_w.at[0]),
        pltpu.make_async_copy(win.at[1], wt.at[d], load_w.at[1]),
    ]
    raw_loads = [
        pltpu.make_async_copy(w.at[0], w_raw.at[k], load_o.at[0, k]) for k, w in enumerate((wv, wg))
    ]
    wo_loads = [
        pltpu.make_async_copy(w.at[1], wo.at[y, k], load_o.at[1, k]) for k, w in enumerate((wv, wg))
    ]
    small = [(decay, decay_v), (freq, freq_v), (step, step_v), (sin, sin_v), (rdo, rdo_v),
             (skip, skip_v)]
    small_loads = [
        pltpu.make_async_copy(src, dst, load.at[i]) for i, (src, dst) in enumerate(small)
    ]
    gain_load = pltpu.make_async_copy(gain, gain_v, load.at[6])
    st_load = pltpu.make_async_copy(st, st_v, load_st.at[0])
    for copy in [win_loads[0], tok_load, win_loads[1], gain_load] + wo_loads + small_loads + [
        st_load
    ] + raw_loads:
        copy.start()

    plane = [(i, k) for i in range(4) for k in range(4) if i + k]
    plane.sort(key=lambda ik: -(min(ik[0], 4 - ik[0]) + min(ik[1], 4 - ik[1])))

    def peer_of(i, k):
        return device((z + i) % 4, (y + k) % 4, x, c)

    sends = Sends()
    win_loads[0].wait()
    tok_load.wait()
    gain_load.wait()
    gain_all[d] = gain_v[1:2]
    pl.semaphore_wait(barrier, len(greeted))

    for i in (2, 1, 3):
        sends.go(wi.at[0], wi.at[i], w_s.at[i], w_r.at[i], device((z + i) % 4, y, x, c))
    for i in (2, 1, 3):
        sends.go(xg.at[y], xg.at[y], a_s.at[i], a_r.at[y], device(z, (y + i) % 4, x, c))
    for i in (2, 1, 3):
        pl.semaphore_signal(near_sem, inc=1, device_id=peer_of(i, 0), device_id_type=MESH)
    win_loads[1].wait()
    for i in (2, 1, 3):
        sends.go(wt.at[d], wt.at[d], t_s.at[i], t_r.at[d], device(z, y, (x + i) % 4, c))
    for i in (2, 1, 3, 0):
        for k in range(2):
            if i + k:
                sends.go(gain_all.at[d], gain_all.at[d], g_s.at[i * 2 + k], g_r.at[d],
                         device(z, y, (x + i) % 4, (c + k) % 2))
    for copy in wo_loads:
        copy.wait()
    for i in (2, 1, 3):
        sends.go(wo.at[y], wo.at[y], o_s.at[i], o_r.at[y], device(z, (y + i) % 4, x, c))

    for copy in small_loads:
        copy.wait()
    rate = jnp.concatenate([decay_v[0], decay_v[1]], axis=0)
    often = jnp.concatenate([freq_v[0], freq_v[1]], axis=0)
    steps = step_v[...]
    times = jnp.concatenate(
        [jnp.broadcast_to(steps[l:l + 1, g:g + 1], (1, 64)) for l in range(L) for g in range(4)],
        axis=0,
    )
    magnitude = jnp.exp(-rate * times)
    angle = often * times
    keep_r = magnitude * jnp.cos(angle)
    keep_i = magnitude * jnp.sin(angle)
    minus = keep_r - 1.0
    below = rate * rate + often * often
    lift_r = (-minus * rate + keep_i * often) / below
    lift_i = (-keep_i * rate - minus * often) / below
    keep_r = jnp.concatenate([keep_r, keep_r], axis=1)
    keep_i = jnp.concatenate([-keep_i, keep_i], axis=1)
    lift_r = jnp.concatenate([lift_r, lift_r], axis=1)
    lift_i = jnp.concatenate([-lift_i, lift_i], axis=1)

    rows = lax.broadcasted_iota(jnp.int32, (128, 128), 0)
    lanes = lax.broadcasted_iota(jnp.int32, (128, 128), 1)
    same_group = rows // 16 == lanes // 16
    lane16 = lax.broadcasted_iota(jnp.int32, (16, 128), 1)
    row16 = lax.broadcasted_iota(jnp.int32, (16, 128), 0)
    low = lane16 < 64

    st_load.wait()

    def prepare(l):
        lifted = []
        for g in range(4):
            k = l * 4 + g
            b = sin_v[l, g]
            lifted.append(lift_r[k:k + 1] * b + lift_i[k:k + 1] * pltpu.roll(b, 64, 1))
        both = jnp.concatenate(lifted + lifted, axis=0)
        big_b[l] = both
        out = jnp.concatenate([rdo_v[l, g] for g in range(4)] * 2, axis=0)
        skips = jnp.concatenate([skip_v[l:l + 1], skip_v[l:l + 1]], axis=1)
        m = jnp.where(same_group, nt(both, out, HIGH), 0.0)
        m = m + jnp.where(rows == lanes, jnp.broadcast_to(skips, (128, 128)), 0.0)
        hi = m.astype(BF16)
        m3[l] = jnp.concatenate([hi, hi, (m - hi.astype(F32)).astype(BF16)], axis=0)
        for g in range(4):
            k = l * 4 + g
            s = st_v[l, :, g, :]
            kept = keep_r[k:k + 1] * s + keep_i[k:k + 1] * pltpu.roll(s, 64, 1)
            ks[l, g * 2] = kept[:16]
            ks[l, g * 2 + 1] = kept[16:]
        prod = nt(ks[l].reshape(128, 128), out, HIGH)
        total = jnp.zeros((16, 128), F32)
        for g in range(4):
            for h in range(2):
                block = prod[(g * 2 + h) * 16:(g * 2 + h) * 16 + 16]
                total = total + jnp.where(lane16 // 16 == h * 4 + g, block, 0.0)
        base[l] = total

    prepare(0)
    pl.semaphore_wait(near_sem, 3)
    for i in (2, 1, 3):
        pl.semaphore_signal(far_sem, inc=1, device_id=peer_of(0, i), device_id_type=MESH)
    prepare(1)

    def read_out(l, raw, scale):
        hi = raw.astype(BF16)
        lo = (raw - hi.astype(F32)).astype(BF16)
        mixed = jnp.dot(
            jnp.concatenate([hi, lo, hi], axis=1), m3[l], preferred_element_type=F32
        )
        return jax.nn.gelu(base[l] + scale * mixed)

    def new_states(l, drive):
        pieces = [
            jnp.where(lane16 // 16 == h * 4 + g, drive, 0.0) for g in range(4) for h in range(2)
        ]
        push = jnp.dot(
            jnp.concatenate(pieces, axis=0), big_b[l], precision=HIGH, preferred_element_type=F32
        )
        for g in range(4):
            for h in range(2):
                k = g * 2 + h
                new_v[l, h * 16:h * 16 + 16, g, :] = ks[l, k] + push[k * 16:k * 16 + 16]
        pltpu.make_async_copy(new_v.at[l], st_out.at[l], done.at[l]).start()

    for k in range(4):
        @pl.when(y != k)
        def _(k=k):
            arrived(xg.at[k], a_r.at[k])
    wide = xg[...].reshape(64, 512).astype(F32)
    gained = (wide * gain_v[0:1]).astype(BF16)
    square = jnp.sum(wide * wide, axis=1, keepdims=True)
    row32 = lax.broadcasted_iota(jnp.int32, (32, 128), 0)
    lane32 = lax.broadcasted_iota(jnp.int32, (32, 128), 1)
    for k in range(2):
        part_sq = jnp.where(row32 == lane32, square[k * 32:k * 32 + 32], 0.0)
        sq[k] = jnp.broadcast_to(jnp.sum(part_sq, axis=0, keepdims=True), (8, 128))

    pl.semaphore_wait(far_sem, 3)

    def send_w0(k):
        raw_loads[k].wait()
        for i in (2, 1, 3, 0):
            for j in range(2):
                here = None
                if i == 0:
                    here = (z == x) & (y == 2 * c + j) & (y % 2 == c)
                sends.go(w_raw.at[k, :, pl.ds(j * 256, 256)], w0.at[t, k],
                         h_s.at[k, i * 2 + j], h_r.at[t, k],
                         device(x, 2 * c + j, (x + i) % 4, y % 2), here)

    send_w0(0)
    for i in (0, 1, 3, 2):
        if i:
            arrived(wi.at[i], w_r.at[i])
        prod = nt(gained, jnp.concatenate([wi[i], wi[i]], axis=0))
        for k in range(2):
            upper = prod[k * 32:k * 32 + 16]
            lower = prod[k * 32 + 16:k * 32 + 32]
            pb[i, k] = jnp.where(low, upper, lower).astype(BF16)
        for k in range(2):
            to = device((z - i) % 4, y, z, k)
            here = None if i else (x == z) & (c == k)
            sends.go(pb.at[i, k], bm.at[d], b_s.at[i * 2 + k], b_r.at[d], to, here)
            sends.go(sq.at[k], bq.at[d], q_s.at[i * 2 + k], q_r.at[d], to, here)
    send_w0(1)
    for j in range(2):
        here = (z == x) & (y == 2 * c + j)
        sends.go(xg.at[y, :, pl.ds(j * 256, 256)], res0.at[y % 2], e_s.at[0, j],
                 e_r.at[0, y % 2], device(x, 2 * c + j, z, y // 2), here)
    for i in range(4):
        k = ((x + i) % 4) * 2 + c
        if i:
            arrived(wt.at[k], t_r.at[k])
        sends.go(wt.at[k], wt.at[k], tf_s.at[i], t_r.at[k], device(z, y, x, other))

    for k in range(8):
        arrived(bq.at[k], q_r.at[k])
        arrived(bm.at[k], b_r.at[k])
    squares = bq[0]
    raw = bm[0].astype(F32)
    for k in range(1, 8):
        squares = squares + bq[k]
        raw = raw + bm[k].astype(F32)
    spread = jnp.broadcast_to(squares[0:1], (16, 128))
    first = jnp.sum(jnp.where(lane16 == row16, spread, 0.0), axis=1, keepdims=True)
    second = jnp.sum(jnp.where(lane16 == row16 + 16, spread, 0.0), axis=1, keepdims=True)
    scale = lax.rsqrt(jnp.where(low, first, second) * (1.0 / D) + EPS)
    side = y % 2
    ready = read_out(0, raw, scale)
    rg[t] = jnp.where(side == 0, ready, pltpu.roll(ready, 64, 1)).astype(BF16)
    for i, k in plane:
        sends.go(rg.at[t], rg.at[t], k_s.at[i * 4 + k], k_r.at[t], peer_of(i, k))

    for k in range(2):
        for i in range(8):
            s = (i // 2) * 4 + (i % 2) * 2 + c
            arrived(w0.at[s, k], h_r.at[s, k])
            sends.go(w0.at[s, k], w0.at[s, k], hf_s.at[k, i], h_r.at[s, k],
                     device(z, y, x, other))
    new_states(0, scale * raw)
    for k in range(2):
        for i in range(8):
            s = (i // 2) * 4 + (i % 2) * 2 + other
            arrived(w0.at[s, k], h_r.at[s, k])
    for k in range(2):
        arrived(res0.at[k], e_r.at[0, k])
    for k in range(16):
        @pl.when(t != k)
        def _(k=k):
            arrived(rg.at[k], k_r.at[k])
    chunks = []
    for k in range(0, 16, 2):
        even, odd = rg[k], rg[k + 1]
        top = jnp.where(low, even, odd)
        bottom = jnp.where(low, odd, even)
        bottom = jnp.concatenate([bottom[:, 64:], bottom[:, :64]], axis=1)
        chunks.append(jnp.concatenate([top, bottom], axis=0))
    left = jnp.concatenate(chunks, axis=1)
    value = jnp.dot(left, w0[:, 0].reshape(1024, 256), preferred_element_type=F32)
    gate = jnp.dot(left, w0[:, 1].reshape(1024, 256), preferred_element_type=F32)
    current = res0[...].reshape(32, 256).astype(F32) + value * jax.nn.sigmoid(gate)
    xa[t] = current.astype(BF16)
    for i, k in plane:
        sends.go(xa.at[t], xa.at[t], n_s.at[i * 4 + k], n_r.at[t], peer_of(i, k))
    for j in range(2):
        here = (z == x) & (y == 2 * c + j)
        sends.go(xa.at[t, pl.ds(j * 16, 16)], res1.at[y % 2], e_s.at[1, j],
                 e_r.at[1, y % 2], device(x, 2 * c + j, z, y // 2), here)

    for k in range(8):
        @pl.when(d != k)
        def _(k=k):
            arrived(gain_all.at[k], g_r.at[k])
    for i in range(4):
        arrived(wt.at[2 * i + other], t_r.at[2 * i + other])
    for k in range(16):
        @pl.when(t != k)
        def _(k=k):
            arrived(xa.at[k], n_r.at[k])
    total = jnp.zeros((32, 128), F32)
    square = jnp.zeros((32, 256), F32)
    for k in range(16):
        half = slice((k % 2) * 256, (k % 2) * 256 + 256)
        wide = xa[k].astype(F32)
        square = square + wide * wide
        gained = (wide * gain_all[k // 2, :, half]).astype(BF16)
        w = wt[k // 2, :, half]
        total = total + nt(gained, jnp.concatenate([w, w], axis=0))
    square = jnp.sum(square, axis=1, keepdims=True)
    raw = jnp.where(low, total[:16], total[16:])
    scale = lax.rsqrt(jnp.where(low, square[:16], square[16:]) * (1.0 / D) + EPS)
    ready = read_out(1, raw, scale)
    turned = pltpu.roll(ready, 64, 1)
    for h in range(2):
        placed = jnp.where(side == h, ready, turned)
        cs[h] = jnp.where(lane16 // 64 == side, placed, 0.0).astype(BF16)
    for h in range(2):
        yy = 2 * c + h
        for i in (2, 1, 3, 0):
            for k in range(2):
                here = y == yy if i + k == 0 else None
                sends.go(cs.at[h], cr.at[x, y], c_s.at[h * 8 + i * 2 + k],
                         c_r.at[x, y], device(z, yy, (x + i) % 4, (c + k) % 2), here)
    new_states(1, scale * raw)

    for k in range(4):
        @pl.when(y != k)
        def _(k=k):
            arrived(wo.at[k], o_r.at[k])
    for k in range(2):
        arrived(res1.at[k], e_r.at[1, k])
    for i in range(4):
        for k in range(4):
            arrived(cr.at[i, k], c_r.at[i, k])
    left = jnp.concatenate(
        [(cr[:, 2 * j] + cr[:, 2 * j + 1]).reshape(64, 128) for j in range(2)], axis=1
    )
    for k in range(2):
        prod = jnp.dot(left, wo[:, k].reshape(256, 512), preferred_element_type=F32)
        for i in range(4):
            part[i, k] = prod[i * 16:i * 16 + 16]
            rs[i, k] = prod[i * 16:i * 16 + 16].astype(BF16)
    for i in (2, 1, 3):
        zz = (z + i) % 4
        sends.go(rs.at[zz], rr.at[i], r_s.at[i], r_r.at[i], device(zz, y, x, c))
    value, gate = part[z, 0], part[z, 1]
    for i in (1, 3, 2):
        arrived(rr.at[i], r_r.at[i])
        value = value + rr[i, 0].astype(F32)
        gate = gate + rr[i, 1].astype(F32)
    before = jnp.concatenate([res1[0], res1[1]], axis=1).astype(F32)
    out_v[...] = (before + value * jax.nn.sigmoid(gate)).astype(BF16)
    copy = pltpu.make_async_copy(out_v, tok_out, done.at[L])
    copy.start()
    sends.finish()
    copy.wait()
    for l in range(L):
        pltpu.make_async_copy(new_v.at[l], st_out.at[l], done.at[l]).wait()


def body(*args):
    args = list(args)
    args[2] = jnp.swapaxes(args[2], 1, 2)
    dma = pltpu.SemaphoreType.DMA
    v = pltpu.VMEM
    anywhere = pl.BlockSpec(memory_space=pl.ANY)
    scratch = [
        v((4, 16, 512), BF16),
        v((4, 64, 512), BF16),
        v((8, 64, 512), BF16),
        v((2, 64, 512), BF16),
        v((16, 2, 64, 256), BF16),
        v((4, 2, 64, 512), BF16),
        v((L, 512), F32),
        v((8, 1, 512), F32),
        v((L, 4, 64), F32),
        v((L, 4, 64), F32),
        v((L, 4), F32),
        v((L, 4, 16, 128), F32),
        v((L, 4, 16, 128), F32),
        v((L, 64), F32),
        v((L, 32, 4, 128), F32),
        v((L, 128, 128), F32),
        v((L, 384, 128), BF16),
        v((L, 16, 128), F32),
        v((L, 8, 16, 128), F32),
        v((4, 2, 16, 128), BF16),
        v((2, 8, 128), F32),
        v((8, 16, 128), BF16),
        v((8, 8, 128), F32),
        v((16, 16, 128), BF16),
        v((2, 16, 256), BF16),
        v((16, 32, 256), BF16),
        v((2, 16, 256), BF16),
        v((2, 16, 128), BF16),
        v((4, 4, 16, 128), BF16),
        v((4, 2, 16, 512), F32),
        v((4, 2, 16, 512), BF16),
        v((4, 2, 16, 512), BF16),
        v((L, 32, 4, 128), F32),
        v((16, 512), BF16),
        dma((7,)), dma((1,)), dma((2,)), dma((2, 2)), dma((1,)),
        dma((4,)), dma((4,)),
        dma((4,)), dma((4,)),
        dma((4,)), dma((4,)),
        dma((8,)), dma((8,)),
        dma((8,)), dma((8,)),
        dma((16,)), dma((4, 4)),
        dma((4,)), dma((4,)),
        dma((4,)), dma((8,)), dma((4,)),
        dma((8,)), dma((8,)),
        dma((2, 8)), dma((16, 2)), dma((2, 8)),
        dma((16,)), dma((16,)),
        dma((16,)), dma((16,)),
        dma((2, 2)), dma((2, 2)),
        pltpu.SemaphoreType.REGULAR,
        pltpu.SemaphoreType.REGULAR,
        dma((L + 1,)),
    ]
    return pl.pallas_call(
        kernel,
        out_shape=(
            jax.ShapeDtypeStruct((16, 512), BF16),
            jax.ShapeDtypeStruct((L, 32, 4, 128), F32),
        ),
        in_specs=[anywhere] * 12,
        out_specs=(anywhere, anywhere),
        scratch_shapes=scratch,
        compiler_params=pltpu.CompilerParams(collective_id=0, has_side_effects=True),
        name="layers",
    )(*args)


def solution(mesh):
    in_specs = (
        P("tp", "dp"),
        P(None, "dp"),
        P(None, "dp", "tp"),
        P(None, "tp", None),
        P(None, "tp", None),
        P(None, "tp"),
        P(None, "tp", None, None),
        P(None, "tp", None, None),
        P(None, "tp"),
        P(None, "tp", "dp"),
        P(None, "tp", "dp"),
        P(None, "dp", "tp", None),
    )
    out_specs = (P("tp", "dp"), P(None, "dp", "tp", None))
    return jax.shard_map(body, mesh=mesh, in_specs=in_specs, out_specs=out_specs, check_vma=False)
```

```python
import jax
import jax.numpy as jnp
from jax import lax
from jax.experimental import pallas as pl
from jax.experimental.pallas import tpu as pltpu
from jax.sharding import PartitionSpec as P

D = 4096
L = 2
EPS = 1e-06
MESH = pl.DeviceIdType.MESH
F32 = jnp.float32
BF16 = jnp.bfloat16
HIGH = lax.Precision.HIGHEST


def nt(a, b, precision=None):
    return lax.dot_general(
        a, b, (((1,), (1,)), ((), ())), precision=precision, preferred_element_type=F32
    )


def device(z, y, x, c):
    return (z * 4 + y, x * 2 + c)


class Sends:
    def __init__(self):
        self.waits = []

    def go(self, src, dst, send_sem, recv_sem, to, here=None):
        copy = pltpu.make_async_remote_copy(
            src_ref=src, dst_ref=dst, send_sem=send_sem, recv_sem=recv_sem,
            device_id=to, device_id_type=MESH,
        )
        if here is None:
            copy.start()
            self.waits.append((None, copy))
            return

        @pl.when(here)
        def _():
            pltpu.make_async_copy(src, dst, recv_sem).start()

        @pl.when(jnp.logical_not(here))
        def _():
            copy.start()

        self.waits.append((jnp.logical_not(here), copy))

    def finish(self):
        for away, copy in self.waits:
            if away is None:
                copy.wait_send()
            else:
                @pl.when(away)
                def _(copy=copy):
                    copy.wait_send()


def arrived(dst, sem):
    pltpu.make_async_copy(dst, dst, sem).wait()


def waited(ref, sem, k):
    arrived(ref.at[k], sem.at[k])
    return ref[k]


def kernel(
    tok, gain, win, decay, freq, step, sin, rdo, skip, wv, wg, st,
    tok_out, st_out,
    xg, wi, wt, w_raw, wy, wz, w0, wp, gain_p, wo, gain_v, gain_all, decay_v, freq_v, step_v, sin_v, rdo_v, skip_v, st_v,
    big_b, m3, base, ks, pb, sq, bm, bq, rg, res0, rest, xa, res1, cs, cr, part, rs, rr,
    load, load_st, load_w, load_o, load_x, load_r, a_s, a_r, w_s, w_r, o_s, o_r,
    b_s, b_r, q_s, q_r, c_s, c_r, r_s, r_r, t_s, t_r, tf_s, g_s, g_r, h_s, h_r, hf_s, hx_r,
    k_s, k_r, n_s, n_r, e_s, e_r,
):
    t, d = lax.axis_index("tp"), lax.axis_index("dp")
    z, y, x, c = t // 4, t % 4, d // 2, d % 2
    other = 1 - c
    barrier = pltpu.get_barrier_semaphore()
    greeted = [(z, (y + i) % 4, x, c) for i in (1, 2, 3)]
    greeted += [((z + i) % 4, y, x, c) for i in (1, 2, 3)]
    greeted += [(z, y, (x + i) % 4, (c + k) % 2) for i in range(4) for k in range(2) if i + k]
    for peer in greeted:
        pl.semaphore_signal(barrier, inc=1, device_id=device(*peer), device_id_type=MESH)

    tok_load = pltpu.make_async_copy(tok, xg.at[y], load_x.at[0])
    win_loads = [
        pltpu.make_async_copy(win.at[0], wi.at[0], load_w.at[0]),
        pltpu.make_async_copy(win.at[1], wt.at[d], load_w.at[1]),
    ]
    raw_loads = [
        pltpu.make_async_copy(w.at[0, :, pl.ds(i * 128, 128)], w_raw.at[i, k], load_r.at[i * 2 + k])
        for i in range(4) for k, w in enumerate((wv, wg))
    ]
    wo_loads = [
        pltpu.make_async_copy(w.at[1], wo.at[y, k], load_o.at[1, k]) for k, w in enumerate((wv, wg))
    ]
    small = [(decay, decay_v), (freq, freq_v), (step, step_v), (sin, sin_v), (rdo, rdo_v),
             (skip, skip_v)]
    small_loads = [
        pltpu.make_async_copy(src, dst, load.at[i]) for i, (src, dst) in enumerate(small)
    ]
    gain_load = pltpu.make_async_copy(gain, gain_v, load.at[6])
    st_load = pltpu.make_async_copy(st, st_v, load_st.at[0])
    for copy in [win_loads[0], tok_load, gain_load] + raw_loads + [win_loads[1]] + small_loads + [
        st_load
    ] + wo_loads:
        copy.start()

    plane = [(i, k) for i in range(4) for k in range(4) if i + k]
    plane.sort(key=lambda ik: -(min(ik[0], 4 - ik[0]) + min(ik[1], 4 - ik[1])))

    def peer_of(i, k):
        return device((z + i) % 4, (y + k) % 4, x, c)

    sends = Sends()
    win_loads[0].wait()
    tok_load.wait()
    gain_load.wait()
    gain_all[d] = gain_v[1:2]
    pl.semaphore_wait(barrier, len(greeted))

    for i in (2, 1, 3):
        sends.go(wi.at[0], wi.at[i], w_s.at[i], w_r.at[i], device((z + i) % 4, y, x, c))
    for i in (2, 1, 3):
        sends.go(xg.at[y], xg.at[y], a_s.at[i], a_r.at[y], device(z, (y + i) % 4, x, c))
    for copy in raw_loads:
        copy.wait()
    for i in (2, 1, 3):
        yy = (y + i) % 4
        sends.go(w_raw.at[yy], wy.at[y], h_s.at[i], h_r.at[y], device(z, yy, x, c))
    win_loads[1].wait()
    for i in (2, 1, 3):
        sends.go(wt.at[d], wt.at[d], t_s.at[i], t_r.at[d], device(z, y, (x + i) % 4, c))
    for i in (2, 1, 3, 0):
        for k in range(2):
            if i + k:
                sends.go(gain_all.at[d], gain_all.at[d], g_s.at[i * 2 + k], g_r.at[d],
                         device(z, y, (x + i) % 4, (c + k) % 2))
    for copy in wo_loads:
        copy.wait()
    for i in (2, 1, 3):
        sends.go(wo.at[y], wo.at[y], o_s.at[i], o_r.at[y], device(z, (y + i) % 4, x, c))

    for copy in small_loads:
        copy.wait()
    rate = jnp.concatenate([decay_v[0], decay_v[1]], axis=0)
    often = jnp.concatenate([freq_v[0], freq_v[1]], axis=0)
    steps = step_v[...]
    times = jnp.concatenate(
        [jnp.broadcast_to(steps[l:l + 1, g:g + 1], (1, 64)) for l in range(L) for g in range(4)],
        axis=0,
    )
    magnitude = jnp.exp(-rate * times)
    angle = often * times
    keep_r = magnitude * jnp.cos(angle)
    keep_i = magnitude * jnp.sin(angle)
    minus = keep_r - 1.0
    below = rate * rate + often * often
    lift_r = (-minus * rate + keep_i * often) / below
    lift_i = (-keep_i * rate - minus * often) / below
    keep_r = jnp.concatenate([keep_r, keep_r], axis=1)
    keep_i = jnp.concatenate([-keep_i, keep_i], axis=1)
    lift_r = jnp.concatenate([lift_r, lift_r], axis=1)
    lift_i = jnp.concatenate([-lift_i, lift_i], axis=1)

    rows = lax.broadcasted_iota(jnp.int32, (128, 128), 0)
    lanes = lax.broadcasted_iota(jnp.int32, (128, 128), 1)
    same_group = rows // 16 == lanes // 16
    lane16 = lax.broadcasted_iota(jnp.int32, (16, 128), 1)
    row16 = lax.broadcasted_iota(jnp.int32, (16, 128), 0)
    low = lane16 < 64

    st_load.wait()

    def prepare(l):
        lifted = []
        for g in range(4):
            k = l * 4 + g
            b = sin_v[l, g]
            lifted.append(lift_r[k:k + 1] * b + lift_i[k:k + 1] * pltpu.roll(b, 64, 1))
        both = jnp.concatenate(lifted + lifted, axis=0)
        big_b[l] = both
        out = jnp.concatenate([rdo_v[l, g] for g in range(4)] * 2, axis=0)
        skips = jnp.concatenate([skip_v[l:l + 1], skip_v[l:l + 1]], axis=1)
        m = jnp.where(same_group, nt(both, out, HIGH), 0.0)
        m = m + jnp.where(rows == lanes, jnp.broadcast_to(skips, (128, 128)), 0.0)
        hi = m.astype(BF16)
        m3[l] = jnp.concatenate([hi, hi, (m - hi.astype(F32)).astype(BF16)], axis=0)
        for g in range(4):
            k = l * 4 + g
            s = st_v[l, :, g, :]
            kept = keep_r[k:k + 1] * s + keep_i[k:k + 1] * pltpu.roll(s, 64, 1)
            ks[l, g * 2] = kept[:16]
            ks[l, g * 2 + 1] = kept[16:]
        prod = nt(ks[l].reshape(128, 128), out, HIGH)
        total = jnp.zeros((16, 128), F32)
        for g in range(4):
            for h in range(2):
                block = prod[(g * 2 + h) * 16:(g * 2 + h) * 16 + 16]
                total = total + jnp.where(lane16 // 16 == h * 4 + g, block, 0.0)
        base[l] = total

    prepare(0)
    prepare(1)

    def read_out(l, raw, scale):
        hi = raw.astype(BF16)
        lo = (raw - hi.astype(F32)).astype(BF16)
        mixed = jnp.dot(
            jnp.concatenate([hi, lo, hi], axis=1), m3[l], preferred_element_type=F32
        )
        return jax.nn.gelu(base[l] + scale * mixed)

    def new_states(l, drive):
        pieces = [
            jnp.where(lane16 // 16 == h * 4 + g, drive, 0.0) for g in range(4) for h in range(2)
        ]
        push = jnp.dot(
            jnp.concatenate(pieces, axis=0), big_b[l], precision=HIGH, preferred_element_type=F32
        )
        for g in range(4):
            for h in range(2):
                k = g * 2 + h
                st_out[l, h * 16:h * 16 + 16, g, :] = ks[l, k] + push[k * 16:k * 16 + 16]

    for k in range(4):
        @pl.when(y != k)
        def _(k=k):
            arrived(xg.at[k], a_r.at[k])
    wide = xg[...].reshape(64, 512).astype(F32)
    gained = (wide * gain_v[0:1]).astype(BF16)
    square = jnp.sum(wide * wide, axis=1, keepdims=True)
    row32 = lax.broadcasted_iota(jnp.int32, (32, 128), 0)
    lane32 = lax.broadcasted_iota(jnp.int32, (32, 128), 1)
    for k in range(2):
        part_sq = jnp.where(row32 == lane32, square[k * 32:k * 32 + 32], 0.0)
        sq[k] = jnp.sum(part_sq, axis=0, keepdims=True)

    wy[y] = w_raw[y]
    for k in range(4):
        @pl.when(y != k)
        def _(k=k):
            arrived(wy.at[k], h_r.at[k])
        turned = jnp.transpose(wy[k].reshape(128, 128).astype(F32)).astype(BF16)
        for i in range(4):
            wz[i, k] = turned[i * 32:i * 32 + 32]
    for i in (2, 1, 3):
        zz = (z + i) % 4
        sends.go(wz.at[zz], w0.at[d, z], h_s.at[4 + i], h_r.at[4 + z], device(zz, y, x, c))
    w0[d, z] = wz[z]

    for i in (0, 1, 3, 2):
        if i:
            arrived(wi.at[i], w_r.at[i])
        prod = nt(gained, jnp.concatenate([wi[i], wi[i]], axis=0))
        for k in range(2):
            upper = prod[k * 32:k * 32 + 16]
            lower = prod[k * 32 + 16:k * 32 + 32]
            pb[i, k] = jnp.where(low, upper, lower).astype(BF16)
        for k in range(2):
            to = device((z - i) % 4, y, z, k)
            here = None if i else (x == z) & (c == k)
            sends.go(pb.at[i, k], bm.at[d], b_s.at[i * 2 + k], b_r.at[d], to, here)
            sends.go(sq.at[k], bq.at[d], q_s.at[i * 2 + k], q_r.at[d], to, here)
    for i in range(4):
        for k in range(2):
            here = None if i else (x == z) & (c == k)
            sends.go(xg.at[pl.ds(2 * k, 2), :, pl.ds(pl.multiple_of(y * 128, 128), 128)], res0.at[d],
                     e_s.at[i * 2 + k], e_r.at[d], device((z - i) % 4, y, z, k), here)
    for i in range(4):
        k = ((x + i) % 4) * 2 + c
        if i:
            arrived(wt.at[k], t_r.at[k])
        sends.go(wt.at[k], wt.at[k], tf_s.at[i], t_r.at[k], device(z, y, x, other))

    for k in range(4):
        @pl.when(z != k)
        def _(k=k):
            arrived(w0.at[d, k], h_r.at[4 + k])
    for i in (2, 1, 3):
        sends.go(w0.at[d], w0.at[d], h_s.at[8 + i], hx_r.at[d], device(z, y, (x + i) % 4, c))
    sends.go(w0.at[d], w0.at[d], hf_s.at[0], hx_r.at[d], device(z, y, x, other))

    for k in range(8):
        arrived(bq.at[k], q_r.at[k])
        arrived(bm.at[k], b_r.at[k])
    squares = bq[0]
    raw = bm[0].astype(F32)
    for k in range(1, 8):
        squares = squares + bq[k]
        raw = raw + bm[k].astype(F32)
    spread = jnp.broadcast_to(squares, (16, 128))
    first = jnp.sum(jnp.where(lane16 == row16, spread, 0.0), axis=1, keepdims=True)
    second = jnp.sum(jnp.where(lane16 == row16 + 16, spread, 0.0), axis=1, keepdims=True)
    scale = lax.rsqrt(jnp.where(low, first, second) * (1.0 / D) + EPS)
    side = y % 2
    ready = read_out(0, raw, scale)
    rg[t] = ready.astype(BF16)
    for i, k in plane:
        sends.go(rg.at[t], rg.at[t], k_s.at[i * 4 + k], k_r.at[t], peer_of(i, k))

    new_states(0, scale * raw)

    lane = lax.broadcasted_iota(jnp.int32, (1, 128), 1) // 32

    def regroup(tiles, first_block, mine):
        out = None
        for a, tile in enumerate(tiles):
            piece = pltpu.roll(tile, 32 * ((mine(a) - first_block(a)) % 4), 1)
            out = piece if out is None else jnp.where(lane == mine(a), piece, out)
        return out

    rest0 = jnp.concatenate(
        [
            regroup([waited(res0, e_r, 4 * g + a).reshape(32, 128).astype(F32) for a in range(4)],
                    lambda a: z, lambda a: a)
            for g in range(2)
        ],
        axis=1,
    )
    for i in range(4):
        arrived(wt.at[2 * i + other], t_r.at[2 * i + other])
    for k in range(8):
        @pl.when(d != k)
        def _(k=k):
            arrived(gain_all.at[k], g_r.at[k])
    for k in range(16):
        tile = slice((k % 4) * 128, (k % 4) * 128 + 128)
        for g in range(2):
            wp[k, g] = regroup(
                [wt[4 * g + a, :, tile].astype(F32) for a in range(4)], lambda a: k // 4, lambda a: a
            ).astype(BF16)
            gain_p[k, :, g * 128:g * 128 + 128] = regroup(
                [gain_all[4 * g + a, :, tile] for a in range(4)], lambda a: k // 4, lambda a: a
            )

    for i in (1, 3, 2):
        k = ((x + i) % 4) * 2 + c
        arrived(w0.at[k], hx_r.at[k])
        sends.go(w0.at[k], w0.at[k], hf_s.at[i], hx_r.at[k], device(z, y, x, other))
    for k in range(16):
        @pl.when(t != k)
        def _(k=k):
            arrived(rg.at[k], k_r.at[k])
    chunks = []
    for k in range(16):
        own = rg[k].astype(F32)
        swapped = pltpu.roll(own, 64, 1)
        chunks.append(jnp.concatenate(
            [jnp.where(low, own, 0.0), jnp.where(low, swapped, 0.0),
             jnp.where(low, 0.0, swapped), jnp.where(low, 0.0, own)], axis=0).astype(BF16))
    for i in range(4):
        arrived(w0.at[2 * i + other], hx_r.at[2 * i + other])
    both = jnp.zeros((64, 256), F32)
    for k in range(16):
        both = both + nt(chunks[k], w0[:, k // 4, k % 4].reshape(256, 128))
    current = rest0 + both[:32] * jax.nn.sigmoid(both[32:])
    xa[t] = current.astype(BF16)
    for i, k in plane:
        sends.go(xa.at[t], xa.at[t], n_s.at[i * 4 + k], n_r.at[t], peer_of(i, k))

    for k in range(16):
        @pl.when(t != k)
        def _(k=k):
            arrived(xa.at[k], n_r.at[k])
    total = jnp.zeros((32, 128), F32)
    square = jnp.zeros((32, 256), F32)
    for k in range(16):
        wide = xa[k].astype(F32)
        square = square + wide * wide
        gained = (wide * gain_p[k]).astype(BF16)
        w = jnp.concatenate([wp[k, 0], wp[k, 1]], axis=1)
        total = total + nt(gained, jnp.concatenate([w, w], axis=0))
    square = jnp.sum(square, axis=1, keepdims=True)
    raw = jnp.where(low, total[:16], total[16:])
    scale = lax.rsqrt(jnp.where(low, square[:16], square[16:]) * (1.0 / D) + EPS)
    ready = read_out(1, raw, scale)
    turned = pltpu.roll(ready, 64, 1)
    for h in range(2):
        placed = jnp.where(side == h, ready, turned)
        cs[h] = jnp.where(lane16 // 64 == side, placed, 0.0).astype(BF16)
    for h in range(2):
        yy = 2 * c + h
        for i in (2, 1, 3, 0):
            for k in range(2):
                here = y == yy if i + k == 0 else None
                sends.go(cs.at[h], cr.at[x, y], c_s.at[h * 8 + i * 2 + k],
                         c_r.at[x, y], device(z, yy, (x + i) % 4, (c + k) % 2), here)
    new_states(1, scale * raw)

    half_to, d_to = z // 2, t % 8
    for k in range(4):
        tiles = []
        for i in range(4):
            piece = xa[i * 4 + k, pl.ds(pl.multiple_of(half_to * 16, 16), 16), :].astype(F32)
            tiles.append(jnp.where(d_to // 4 == 0, piece[:, :128], piece[:, 128:]))
        rest[:, k * 128:k * 128 + 128] = regroup(tiles, lambda a: d_to % 4, lambda a: a).astype(BF16)
    here = (z == x) & (y == 2 * c + half_to) & (d == d_to)
    sends.go(rest, res1, e_s.at[8], e_r.at[8],
             device(x, 2 * c + half_to, d_to // 2, d_to % 2), here)

    for k in range(4):
        @pl.when(y != k)
        def _(k=k):
            arrived(wo.at[k], o_r.at[k])
    for i in range(4):
        for k in range(4):
            arrived(cr.at[i, k], c_r.at[i, k])
    left = jnp.concatenate(
        [(cr[:, 2 * j] + cr[:, 2 * j + 1]).reshape(64, 128) for j in range(2)], axis=1
    )
    for k in range(2):
        prod = jnp.dot(left, wo[:, k].reshape(256, 512), preferred_element_type=F32)
        for i in range(4):
            part[i, k] = prod[i * 16:i * 16 + 16]
            rs[i, k] = prod[i * 16:i * 16 + 16].astype(BF16)
    for i in (2, 1, 3):
        zz = (z + i) % 4
        sends.go(rs.at[zz], rr.at[i], r_s.at[i], r_r.at[i], device(zz, y, x, c))
    value, gate = part[z, 0], part[z, 1]
    for i in (1, 3, 2):
        arrived(rr.at[i], r_r.at[i])
        value = value + rr[i, 0].astype(F32)
        gate = gate + rr[i, 1].astype(F32)
    arrived(res1, e_r.at[8])
    before = res1[...].astype(F32)
    tok_out[...] = (before + value * jax.nn.sigmoid(gate)).astype(BF16)
    sends.finish()


def layers(*args):
    args = list(args)
    args[2] = jnp.swapaxes(args[2], 1, 2)
    dma = pltpu.SemaphoreType.DMA
    v = pltpu.VMEM
    anywhere = pl.BlockSpec(memory_space=pl.ANY)
    scratch = [
        v((4, 16, 512), BF16),
        v((4, 64, 512), BF16),
        v((8, 64, 512), BF16),
        v((4, 2, 64, 128), BF16),
        v((4, 2, 64, 128), BF16),
        v((4, 4, 32, 128), BF16),
        v((8, 4, 4, 32, 128), BF16),
        v((16, 2, 64, 128), BF16),
        v((16, 1, 256), F32),
        v((4, 2, 64, 512), BF16),
        v((L, 512), F32),
        v((8, 1, 512), F32),
        v((L, 4, 64), F32),
        v((L, 4, 64), F32),
        v((L, 4), F32),
        v((L, 4, 16, 128), F32),
        v((L, 4, 16, 128), F32),
        v((L, 64), F32),
        v((L, 32, 4, 128), F32),
        v((L, 128, 128), F32),
        v((L, 384, 128), BF16),
        v((L, 16, 128), F32),
        v((L, 8, 16, 128), F32),
        v((4, 2, 16, 128), BF16),
        v((2, 1, 128), F32),
        v((8, 16, 128), BF16),
        v((8, 1, 128), F32),
        v((16, 16, 128), BF16),
        v((8, 2, 16, 128), BF16),
        v((16, 512), BF16),
        v((16, 32, 256), BF16),
        v((16, 512), BF16),
        v((2, 16, 128), BF16),
        v((4, 4, 16, 128), BF16),
        v((4, 2, 16, 512), F32),
        v((4, 2, 16, 512), BF16),
        v((4, 2, 16, 512), BF16),
        dma((7,)), dma((1,)), dma((2,)), dma((2, 2)), dma((1,)), dma((8,)),
        dma((4,)), dma((4,)),
        dma((4,)), dma((4,)),
        dma((4,)), dma((4,)),
        dma((8,)), dma((8,)),
        dma((8,)), dma((8,)),
        dma((16,)), dma((4, 4)),
        dma((4,)), dma((4,)),
        dma((4,)), dma((8,)), dma((4,)),
        dma((8,)), dma((8,)),
        dma((12,)), dma((12,)), dma((8,)),
        dma((8,)),
        dma((16,)), dma((16,)),
        dma((16,)), dma((16,)),
        dma((9,)), dma((9,)),
    ]
    return pl.pallas_call(
        kernel,
        out_shape=(
            pltpu.VMEM((16, 512), BF16),
            pltpu.VMEM((L, 32, 4, 128), F32),
        ),
        in_specs=[anywhere] * 12,
        out_specs=(pl.BlockSpec(memory_space=pltpu.VMEM),)*2,
        scratch_shapes=scratch,
        compiler_params=pltpu.CompilerParams(collective_id=0, has_side_effects=True),
        name="layers",
    )(*args)


def tail(new_tokens, new_states, tokens_out, states_out, sem):
    copies = [
        pltpu.make_async_copy(new_states, states_out, sem.at[0]),
        pltpu.make_async_copy(new_tokens, tokens_out, sem.at[1]),
    ]
    for copy in copies:
        copy.start()
    for copy in copies:
        copy.wait()


def body(*args):
    vmem = pl.BlockSpec(memory_space=pltpu.VMEM)
    anywhere = pl.BlockSpec(memory_space=pl.ANY)
    results = [pltpu.with_memory_space_constraint(a, pltpu.VMEM) for a in layers(*args)]
    return pl.pallas_call(
        tail,
        out_shape=tuple(jax.ShapeDtypeStruct(a.shape, a.dtype) for a in results),
        in_specs=[vmem] * 2,
        out_specs=(anywhere, anywhere),
        scratch_shapes=[pltpu.SemaphoreType.DMA((2,))],
        name="tail",
    )(*results)


def solution(mesh):
    in_specs = (
        P("tp", "dp"),
        P(None, "dp"),
        P(None, "dp", "tp"),
        P(None, "tp", None),
        P(None, "tp", None),
        P(None, "tp"),
        P(None, "tp", None, None),
        P(None, "tp", None, None),
        P(None, "tp"),
        P(None, "tp", "dp"),
        P(None, "tp", "dp"),
        P(None, "dp", "tp", None),
    )
    out_specs = (P("tp", "dp"), P(None, "dp", "tp", None))
    return jax.shard_map(body, mesh=mesh, in_specs=in_specs, out_specs=out_specs, check_vma=False)
```

```python
import jax
import jax.numpy as jnp
from jax import lax
from jax.experimental import pallas as pl
from jax.experimental.pallas import tpu as pltpu
from jax.sharding import PartitionSpec as P

D = 4096
L = 2
EPS = 1e-06
MESH = pl.DeviceIdType.MESH
F32 = jnp.float32
BF16 = jnp.bfloat16
HIGH = lax.Precision.HIGHEST


def nt(a, b, precision=None):
    return lax.dot_general(
        a, b, (((1,), (1,)), ((), ())), precision=precision, preferred_element_type=F32
    )


def device(z, y, x, c):
    return (z * 4 + y, x * 2 + c)


class Sends:
    def __init__(self):
        self.waits = []

    def go(self, src, dst, send_sem, recv_sem, to, here=None):
        copy = pltpu.make_async_remote_copy(
            src_ref=src, dst_ref=dst, send_sem=send_sem, recv_sem=recv_sem,
            device_id=to, device_id_type=MESH,
        )
        if here is None:
            copy.start()
            self.waits.append((None, copy))
            return

        @pl.when(here)
        def _():
            pltpu.make_async_copy(src, dst, recv_sem).start()

        @pl.when(jnp.logical_not(here))
        def _():
            copy.start()

        self.waits.append((jnp.logical_not(here), copy))

    def finish(self):
        for away, copy in self.waits:
            if away is None:
                copy.wait_send()
            else:
                @pl.when(away)
                def _(copy=copy):
                    copy.wait_send()


def arrived(dst, sem):
    pltpu.make_async_copy(dst, dst, sem).wait()


def waited(ref, sem, k):
    arrived(ref.at[k], sem.at[k])
    return ref[k]


def kernel(
    tok, gain, win, decay, freq, step, sin, rdo, skip, wv, wg, st,
    tok_out, st_out,
    xg, wi, wt, w_raw, wy, wz, w0, wp, gain_p, wo, gain_v, gain_all, decay_v, freq_v, step_v, sin_v, rdo_v, skip_v, st_v,
    big_b, m3, base, ks, pb, sq, bm, bq, rg, res0, rest, xa, rest0, res1, cs, cr, part, rs, rr,
    load, load_st, load_w, load_o, load_x, load_r, a_s, a_r, w_s, w_r, o_s, o_r,
    b_s, b_r, q_s, q_r, c_s, c_r, r_s, r_r, t_s, t_r, tf_s, g_s, g_r, h_s, h_r, hf_s, hx_r,
    k_s, k_r, n_s, n_r, e_s, e_r,
):
    t, d = lax.axis_index("tp"), lax.axis_index("dp")
    z, y, x, c = t // 4, t % 4, d // 2, d % 2
    other = 1 - c
    barrier = pltpu.get_barrier_semaphore()
    greeted = [(z, (y + i) % 4, x, c) for i in (1, 2, 3)]
    greeted += [((z + i) % 4, y, x, c) for i in (1, 2, 3)]
    greeted += [(z, y, (x + i) % 4, (c + k) % 2) for i in range(4) for k in range(2) if i + k]
    for peer in greeted:
        pl.semaphore_signal(barrier, inc=1, device_id=device(*peer), device_id_type=MESH)

    tok_load = pltpu.make_async_copy(tok, xg.at[y], load_x.at[0])
    win_loads = [
        pltpu.make_async_copy(win.at[0], wi.at[0], load_w.at[0]),
        pltpu.make_async_copy(win.at[1], wt.at[d], load_w.at[1]),
    ]
    raw_loads = [
        pltpu.make_async_copy(w.at[0, :, pl.ds(i * 128, 128)], w_raw.at[i, k], load_r.at[i * 2 + k])
        for i in range(4) for k, w in enumerate((wv, wg))
    ]
    wo_loads = [
        pltpu.make_async_copy(w.at[1], wo.at[y, k], load_o.at[1, k]) for k, w in enumerate((wv, wg))
    ]
    small = [(decay, decay_v), (freq, freq_v), (step, step_v), (sin, sin_v), (rdo, rdo_v),
             (skip, skip_v)]
    small_loads = [
        pltpu.make_async_copy(src, dst, load.at[i]) for i, (src, dst) in enumerate(small)
    ]
    gain_load = pltpu.make_async_copy(gain, gain_v, load.at[6])
    st_load = pltpu.make_async_copy(st, st_v, load_st.at[0])
    for copy in [win_loads[0], tok_load, gain_load] + raw_loads + [win_loads[1]] + small_loads + [
        st_load
    ] + wo_loads:
        copy.start()

    plane = [(i, k) for i in range(4) for k in range(4) if i + k]
    plane.sort(key=lambda ik: -(min(ik[0], 4 - ik[0]) + min(ik[1], 4 - ik[1])))

    def peer_of(i, k):
        return device((z + i) % 4, (y + k) % 4, x, c)

    sends = Sends()
    win_loads[0].wait()
    tok_load.wait()
    gain_load.wait()
    gain_all[d] = gain_v[1:2]
    pl.semaphore_wait(barrier, len(greeted))

    for i in (2, 1, 3):
        sends.go(wi.at[0], wi.at[i], w_s.at[i], w_r.at[i], device((z + i) % 4, y, x, c))
    for i in (2, 1, 3):
        sends.go(xg.at[y], xg.at[y], a_s.at[i], a_r.at[y], device(z, (y + i) % 4, x, c))
    for copy in raw_loads:
        copy.wait()
    for i in (2, 1, 3):
        yy = (y + i) % 4
        sends.go(w_raw.at[yy], wy.at[y], h_s.at[i], h_r.at[y], device(z, yy, x, c))
    win_loads[1].wait()
    for i in (2, 1, 3):
        sends.go(wt.at[d], wt.at[d], t_s.at[i], t_r.at[d], device(z, y, (x + i) % 4, c))
    for i in (2, 1, 3, 0):
        for k in range(2):
            if i + k:
                sends.go(gain_all.at[d], gain_all.at[d], g_s.at[i * 2 + k], g_r.at[d],
                         device(z, y, (x + i) % 4, (c + k) % 2))

    def send_wo(k):
        wo_loads[k].wait()
        for i in (2, 1, 3):
            sends.go(wo.at[y, k], wo.at[y, k], o_s.at[k, i], o_r.at[k, y],
                     device(z, (y + i) % 4, x, c))

    for copy in small_loads:
        copy.wait()
    rate = jnp.concatenate([decay_v[0], decay_v[1]], axis=0)
    often = jnp.concatenate([freq_v[0], freq_v[1]], axis=0)
    steps = step_v[...]
    times = jnp.concatenate(
        [jnp.broadcast_to(steps[l:l + 1, g:g + 1], (1, 64)) for l in range(L) for g in range(4)],
        axis=0,
    )
    magnitude = jnp.exp(-rate * times)
    angle = often * times
    keep_r = magnitude * jnp.cos(angle)
    keep_i = magnitude * jnp.sin(angle)
    minus = keep_r - 1.0
    below = rate * rate + often * often
    lift_r = (-minus * rate + keep_i * often) / below
    lift_i = (-keep_i * rate - minus * often) / below
    keep_r = jnp.concatenate([keep_r, keep_r], axis=1)
    keep_i = jnp.concatenate([-keep_i, keep_i], axis=1)
    lift_r = jnp.concatenate([lift_r, lift_r], axis=1)
    lift_i = jnp.concatenate([-lift_i, lift_i], axis=1)

    rows = lax.broadcasted_iota(jnp.int32, (128, 128), 0)
    lanes = lax.broadcasted_iota(jnp.int32, (128, 128), 1)
    same_group = rows // 16 == lanes // 16
    lane16 = lax.broadcasted_iota(jnp.int32, (16, 128), 1)
    row16 = lax.broadcasted_iota(jnp.int32, (16, 128), 0)
    low = lane16 < 64

    st_load.wait()

    def prepare(l):
        lifted = []
        for g in range(4):
            k = l * 4 + g
            b = sin_v[l, g]
            lifted.append(lift_r[k:k + 1] * b + lift_i[k:k + 1] * pltpu.roll(b, 64, 1))
        both = jnp.concatenate(lifted + lifted, axis=0)
        big_b[l] = both
        out = jnp.concatenate([rdo_v[l, g] for g in range(4)] * 2, axis=0)
        skips = jnp.concatenate([skip_v[l:l + 1], skip_v[l:l + 1]], axis=1)
        m = jnp.where(same_group, nt(both, out, HIGH), 0.0)
        m = m + jnp.where(rows == lanes, jnp.broadcast_to(skips, (128, 128)), 0.0)
        hi = m.astype(BF16)
        m3[l] = jnp.concatenate([hi, hi, (m - hi.astype(F32)).astype(BF16)], axis=0)
        for g in range(4):
            k = l * 4 + g
            s = st_v[l, :, g, :]
            kept = keep_r[k:k + 1] * s + keep_i[k:k + 1] * pltpu.roll(s, 64, 1)
            ks[l, g * 2] = kept[:16]
            ks[l, g * 2 + 1] = kept[16:]
        prod = nt(ks[l].reshape(128, 128), out, HIGH)
        total = jnp.zeros((16, 128), F32)
        for g in range(4):
            for h in range(2):
                block = prod[(g * 2 + h) * 16:(g * 2 + h) * 16 + 16]
                total = total + jnp.where(lane16 // 16 == h * 4 + g, block, 0.0)
        base[l] = total

    prepare(0)
    prepare(1)

    def read_out(l, raw, scale):
        hi = raw.astype(BF16)
        lo = (raw - hi.astype(F32)).astype(BF16)
        mixed = jnp.dot(
            jnp.concatenate([hi, lo, hi], axis=1), m3[l], preferred_element_type=F32
        )
        return jax.nn.gelu(base[l] + scale * mixed)

    def new_states(l, drive):
        pieces = [
            jnp.where(lane16 // 16 == h * 4 + g, drive, 0.0) for g in range(4) for h in range(2)
        ]
        push = jnp.dot(
            jnp.concatenate(pieces, axis=0), big_b[l], precision=HIGH, preferred_element_type=F32
        )
        for g in range(4):
            for h in range(2):
                k = g * 2 + h
                st_out[l, h * 16:h * 16 + 16, g, :] = ks[l, k] + push[k * 16:k * 16 + 16]

    for k in range(4):
        @pl.when(y != k)
        def _(k=k):
            arrived(xg.at[k], a_r.at[k])
    wide = xg[...].reshape(64, 512).astype(F32)
    gained = (wide * gain_v[0:1]).astype(BF16)
    square = jnp.sum(wide * wide, axis=1, keepdims=True)
    row32 = lax.broadcasted_iota(jnp.int32, (32, 128), 0)
    lane32 = lax.broadcasted_iota(jnp.int32, (32, 128), 1)
    for k in range(2):
        part_sq = jnp.where(row32 == lane32, square[k * 32:k * 32 + 32], 0.0)
        sq[k] = jnp.sum(part_sq, axis=0, keepdims=True)

    wy[y] = w_raw[y]
    for k in range(4):
        @pl.when(y != k)
        def _(k=k):
            arrived(wy.at[k], h_r.at[k])
        turned = jnp.transpose(wy[k].reshape(128, 128).astype(F32)).astype(BF16)
        for i in range(4):
            wz[i, k] = turned[i * 32:i * 32 + 32]
    for i in (2, 1, 3):
        zz = (z + i) % 4
        sends.go(wz.at[zz], w0.at[c, x, z], h_s.at[4 + i], h_r.at[4 + z], device(zz, y, x, c))
    w0[c, x, z] = wz[z]
    send_wo(0)
    send_wo(1)

    for i in (0, 1, 3, 2):
        if i:
            arrived(wi.at[i], w_r.at[i])
        prod = nt(gained, jnp.concatenate([wi[i], wi[i]], axis=0))
        for k in range(2):
            upper = prod[k * 32:k * 32 + 16]
            lower = prod[k * 32 + 16:k * 32 + 32]
            pb[i, k] = jnp.where(low, upper, lower).astype(BF16)
        for k in range(2):
            to = device((z - i) % 4, y, z, k)
            here = None if i else (x == z) & (c == k)
            sends.go(pb.at[i, k], bm.at[d], b_s.at[i * 2 + k], b_r.at[d], to, here)
            sends.go(sq.at[k], bq.at[d], q_s.at[i * 2 + k], q_r.at[d], to, here)
    for i in range(4):
        k = ((x + i) % 4) * 2 + c
        if i:
            arrived(wt.at[k], t_r.at[k])
        sends.go(wt.at[k], wt.at[k], tf_s.at[i], t_r.at[k], device(z, y, x, other))

    for k in range(4):
        @pl.when(z != k)
        def _(k=k):
            arrived(w0.at[c, x, k], h_r.at[4 + k])
    for i in range(4):
        for k in range(2):
            here = None if i else (x == z) & (c == k)
            sends.go(xg.at[pl.ds(2 * k, 2), :, pl.ds(pl.multiple_of(y * 128, 128), 128)], res0.at[d],
                     e_s.at[i * 2 + k], e_r.at[d], device((z - i) % 4, y, z, k), here)
    for i in (2, 1, 3):
        sends.go(w0.at[c, x], w0.at[c, x], h_s.at[8 + i], hx_r.at[c, x], device(z, y, (x + i) % 4, c))
    sends.go(w0.at[c, x], w0.at[c, x], hf_s.at[0], hx_r.at[c, x], device(z, y, x, other))

    for k in range(8):
        arrived(bq.at[k], q_r.at[k])
        arrived(bm.at[k], b_r.at[k])
    squares = bq[0]
    raw = bm[0].astype(F32)
    for k in range(1, 8):
        squares = squares + bq[k]
        raw = raw + bm[k].astype(F32)
    spread = jnp.broadcast_to(squares, (16, 128))
    first = jnp.sum(jnp.where(lane16 == row16, spread, 0.0), axis=1, keepdims=True)
    second = jnp.sum(jnp.where(lane16 == row16 + 16, spread, 0.0), axis=1, keepdims=True)
    scale = lax.rsqrt(jnp.where(low, first, second) * (1.0 / D) + EPS)
    side = y % 2
    ready = read_out(0, raw, scale)
    rg[t] = ready.astype(BF16)
    for i, k in plane:
        sends.go(rg.at[t], rg.at[t], k_s.at[i * 4 + k], k_r.at[t], peer_of(i, k))

    new_states(0, scale * raw)

    lane = lax.broadcasted_iota(jnp.int32, (1, 128), 1) // 32

    def regroup(tiles, first_block, mine):
        out = None
        for a, tile in enumerate(tiles):
            piece = pltpu.roll(tile, 32 * ((mine(a) - first_block(a)) % 4), 1)
            out = piece if out is None else jnp.where(lane == mine(a), piece, out)
        return out

    for i in range(4):
        arrived(wt.at[2 * i + other], t_r.at[2 * i + other])
    for k in range(8):
        @pl.when(d != k)
        def _(k=k):
            arrived(gain_all.at[k], g_r.at[k])
    for k in range(16):
        tile = slice((k % 4) * 128, (k % 4) * 128 + 128)
        for g in range(2):
            wp[k, g] = regroup(
                [wt[2 * a + g, :, tile].astype(F32) for a in range(4)], lambda a: k // 4, lambda a: a
            ).astype(BF16)
            gain_p[k, g] = regroup(
                [gain_all[2 * a + g, :, tile] for a in range(4)], lambda a: k // 4, lambda a: a
            )

    for i in (1, 3, 2):
        k = (x + i) % 4
        arrived(w0.at[c, k], hx_r.at[c, k])
        sends.go(w0.at[c, k], w0.at[c, k], hf_s.at[i], hx_r.at[c, k], device(z, y, x, other))
    for g in range(2):
        rest0[g] = regroup(
            [waited(res0, e_r, 2 * a + g).reshape(32, 128).astype(F32) for a in range(4)],
            lambda a: z, lambda a: a,
        )
    for k in range(16):
        @pl.when(t != k)
        def _(k=k):
            arrived(rg.at[k], k_r.at[k])
    chunks = []
    for k in range(16):
        own = rg[k].astype(F32)
        swapped = pltpu.roll(own, 64, 1)
        chunks.append(jnp.concatenate(
            [jnp.where(low, own, 0.0), jnp.where(low, swapped, 0.0),
             jnp.where(low, 0.0, swapped), jnp.where(low, 0.0, own)], axis=0).astype(BF16))
    left = [jnp.concatenate(chunks[k:k + 2], axis=1) for k in range(0, 16, 2)]
    for which in (c, other):
        if which is other:
            for i in range(4):
                arrived(w0.at[other, i], hx_r.at[other, i])
        both = jnp.zeros((64, 128), F32)
        for j in range(8):
            right = [w0[which, :, k // 4, k % 4].reshape(128, 128) for k in (2 * j, 2 * j + 1)]
            both = both + nt(left[j], jnp.concatenate(right, axis=1))
        xa[t, which] = (rest0[which] + both[:32] * jax.nn.sigmoid(both[32:])).astype(BF16)
        for i, k in plane:
            sends.go(xa.at[t, which], xa.at[t, which], n_s.at[which, i * 4 + k],
                     n_r.at[which, t], peer_of(i, k))

    total = jnp.zeros((32, 128), F32)
    square = jnp.zeros((32, 128), F32)
    near_first = [(0, 0)] + plane[::-1]
    for which in (c, other):
        for j in range(0, 16, 2):
            gained, right = [], []
            for i, k in near_first[j:j + 2]:
                s = ((z + i) % 4) * 4 + (y + k) % 4
                if i + k:
                    arrived(xa.at[s, which], n_r.at[which, s])
                wide = xa[s, which].astype(F32)
                square = square + wide * wide
                gained.append((wide * gain_p[s, which]).astype(BF16))
                right.append(wp[s, which])
            right = jnp.concatenate(right, axis=1)
            right = jnp.concatenate([right, right], axis=0)
            total = total + nt(jnp.concatenate(gained, axis=1), right)
    square = jnp.sum(square, axis=1, keepdims=True)
    raw = jnp.where(low, total[:16], total[16:])
    scale = lax.rsqrt(jnp.where(low, square[:16], square[16:]) * (1.0 / D) + EPS)
    ready = read_out(1, raw, scale)
    turned = pltpu.roll(ready, 64, 1)
    for h in range(2):
        placed = jnp.where(side == h, ready, turned)
        cs[h] = jnp.where(lane16 // 64 == side, placed, 0.0).astype(BF16)
    for h in range(2):
        yy = 2 * c + h
        for i in (2, 1, 3, 0):
            for k in range(2):
                here = y == yy if i + k == 0 else None
                sends.go(cs.at[h], cr.at[x, y], c_s.at[h * 8 + i * 2 + k],
                         c_r.at[x, y], device(z, yy, (x + i) % 4, (c + k) % 2), here)
    new_states(1, scale * raw)

    half_to, d_to = z // 2, t % 8
    for k in range(4):
        tiles = []
        for i in range(4):
            tiles.append(
                xa[i * 4 + k, d_to % 2, pl.ds(pl.multiple_of(half_to * 16, 16), 16), :].astype(F32)
            )
        rest[:, k * 128:k * 128 + 128] = regroup(tiles, lambda a: d_to // 2, lambda a: a).astype(BF16)
    here = (z == x) & (y == 2 * c + half_to) & (d == d_to)
    sends.go(rest, res1, e_s.at[8], e_r.at[8],
             device(x, 2 * c + half_to, d_to // 2, d_to % 2), here)

    for k in range(4):
        @pl.when(y != k)
        def _(k=k):
            for i in range(2):
                arrived(wo.at[k, i], o_r.at[i, k])
    for i in range(4):
        for k in range(4):
            arrived(cr.at[i, k], c_r.at[i, k])
    left = jnp.concatenate(
        [(cr[:, 2 * j] + cr[:, 2 * j + 1]).reshape(64, 128) for j in range(2)], axis=1
    )
    for k in range(2):
        prod = jnp.dot(left, wo[:, k].reshape(256, 512), preferred_element_type=F32)
        for i in range(4):
            part[i, k] = prod[i * 16:i * 16 + 16]
            rs[i, k] = prod[i * 16:i * 16 + 16].astype(BF16)
    for i in (2, 1, 3):
        zz = (z + i) % 4
        sends.go(rs.at[zz], rr.at[i], r_s.at[i], r_r.at[i], device(zz, y, x, c))
    value, gate = part[z, 0], part[z, 1]
    for i in (1, 3, 2):
        arrived(rr.at[i], r_r.at[i])
        value = value + rr[i, 0].astype(F32)
        gate = gate + rr[i, 1].astype(F32)
    arrived(res1, e_r.at[8])
    before = res1[...].astype(F32)
    tok_out[...] = (before + value * jax.nn.sigmoid(gate)).astype(BF16)
    sends.finish()


def layers(*args):
    args = list(args)
    args[2] = jnp.swapaxes(args[2], 1, 2)
    dma = pltpu.SemaphoreType.DMA
    v = pltpu.VMEM
    anywhere = pl.BlockSpec(memory_space=pl.ANY)
    scratch = [
        v((4, 16, 512), BF16),
        v((4, 64, 512), BF16),
        v((8, 64, 512), BF16),
        v((4, 2, 64, 128), BF16),
        v((4, 2, 64, 128), BF16),
        v((4, 4, 32, 128), BF16),
        v((2, 4, 4, 4, 32, 128), BF16),
        v((16, 2, 64, 128), BF16),
        v((16, 2, 1, 128), F32),
        v((4, 2, 64, 512), BF16),
        v((L, 512), F32),
        v((8, 1, 512), F32),
        v((L, 4, 64), F32),
        v((L, 4, 64), F32),
        v((L, 4), F32),
        v((L, 4, 16, 128), F32),
        v((L, 4, 16, 128), F32),
        v((L, 64), F32),
        v((L, 32, 4, 128), F32),
        v((L, 128, 128), F32),
        v((L, 384, 128), BF16),
        v((L, 16, 128), F32),
        v((L, 8, 16, 128), F32),
        v((4, 2, 16, 128), BF16),
        v((2, 1, 128), F32),
        v((8, 16, 128), BF16),
        v((8, 1, 128), F32),
        v((16, 16, 128), BF16),
        v((8, 2, 16, 128), BF16),
        v((16, 512), BF16),
        v((16, 2, 32, 128), BF16),
        v((2, 32, 128), F32),
        v((16, 512), BF16),
        v((2, 16, 128), BF16),
        v((4, 4, 16, 128), BF16),
        v((4, 2, 16, 512), F32),
        v((4, 2, 16, 512), BF16),
        v((4, 2, 16, 512), BF16),
        dma((7,)), dma((1,)), dma((2,)), dma((2, 2)), dma((1,)), dma((8,)),
        dma((4,)), dma((4,)),
        dma((4,)), dma((4,)),
        dma((2, 4)), dma((2, 4)),
        dma((8,)), dma((8,)),
        dma((8,)), dma((8,)),
        dma((16,)), dma((4, 4)),
        dma((4,)), dma((4,)),
        dma((4,)), dma((8,)), dma((4,)),
        dma((8,)), dma((8,)),
        dma((12,)), dma((12,)), dma((8,)),
        dma((2, 4)),
        dma((16,)), dma((16,)),
        dma((2, 16)), dma((2, 16)),
        dma((9,)), dma((9,)),
    ]
    return pl.pallas_call(
        kernel,
        out_shape=(
            pltpu.VMEM((16, 512), BF16),
            pltpu.VMEM((L, 32, 4, 128), F32),
        ),
        in_specs=[anywhere] * 12,
        out_specs=(pl.BlockSpec(memory_space=pltpu.VMEM),)*2,
        scratch_shapes=scratch,
        compiler_params=pltpu.CompilerParams(collective_id=0, has_side_effects=True),
        name="layers",
    )(*args)


def tail(new_tokens, new_states, tokens_out, states_out, sem):
    copies = [
        pltpu.make_async_copy(new_states, states_out, sem.at[0]),
        pltpu.make_async_copy(new_tokens, tokens_out, sem.at[1]),
    ]
    for copy in copies:
        copy.start()
    for copy in copies:
        copy.wait()


def body(*args):
    vmem = pl.BlockSpec(memory_space=pltpu.VMEM)
    anywhere = pl.BlockSpec(memory_space=pl.ANY)
    results = [pltpu.with_memory_space_constraint(a, pltpu.VMEM) for a in layers(*args)]
    return pl.pallas_call(
        tail,
        out_shape=tuple(jax.ShapeDtypeStruct(a.shape, a.dtype) for a in results),
        in_specs=[vmem] * 2,
        out_specs=(anywhere, anywhere),
        scratch_shapes=[pltpu.SemaphoreType.DMA((2,))],
        name="tail",
    )(*results)


def solution(mesh):
    in_specs = (
        P("tp", "dp"),
        P(None, "dp"),
        P(None, "dp", "tp"),
        P(None, "tp", None),
        P(None, "tp", None),
        P(None, "tp"),
        P(None, "tp", None, None),
        P(None, "tp", None, None),
        P(None, "tp"),
        P(None, "tp", "dp"),
        P(None, "tp", "dp"),
        P(None, "dp", "tp", None),
    )
    out_specs = (P("tp", "dp"), P(None, "dp", "tp", None))
    return jax.shard_map(body, mesh=mesh, in_specs=in_specs, out_specs=out_specs, check_vma=False)
```

```python
import jax
import jax.numpy as jnp
from jax import lax
from jax.experimental import pallas as pl
from jax.experimental.pallas import tpu as pltpu
from jax.sharding import PartitionSpec as P

D = 4096
L = 2
EPS = 1e-06
MESH = pl.DeviceIdType.MESH
F32 = jnp.float32
BF16 = jnp.bfloat16
HIGH = lax.Precision.HIGHEST


def nt(a, b, precision=None):
    return lax.dot_general(
        a, b, (((1,), (1,)), ((), ())), precision=precision, preferred_element_type=F32
    )


def device(z, y, x, c):
    return (z * 4 + y, x * 2 + c)


class Sends:
    def __init__(self):
        self.waits = []

    def go(self, src, dst, send_sem, recv_sem, to, here=None):
        copy = pltpu.make_async_remote_copy(
            src_ref=src, dst_ref=dst, send_sem=send_sem, recv_sem=recv_sem,
            device_id=to, device_id_type=MESH,
        )
        if here is None:
            copy.start()
            self.waits.append((None, copy))
            return

        @pl.when(here)
        def _():
            pltpu.make_async_copy(src, dst, recv_sem).start()

        @pl.when(jnp.logical_not(here))
        def _():
            copy.start()

        self.waits.append((jnp.logical_not(here), copy))

    def finish(self, but=0):
        last = len(self.waits) - but
        done, self.waits = self.waits[:last], self.waits[last:]
        for away, copy in done:
            if away is None:
                copy.wait_send()
            else:
                @pl.when(away)
                def _(copy=copy):
                    copy.wait_send()


def arrived(dst, sem):
    pltpu.make_async_copy(dst, dst, sem).wait()


def waited(ref, sem, k):
    arrived(ref.at[k], sem.at[k])
    return ref[k]


def kernel(
    tok, gain, win, decay, freq, step, sin, rdo, skip, wv, wg, st,
    tok_out, st_out,
    xg, wi, wt, w_raw, wy, wz, w0, wp, gain_p, wo, gain_v, gain_all, decay_v, freq_v, step_v, sin_v, rdo_v, skip_v, st_v,
    big_b, m3, base, ks, pb, sq, bm, bq, rg, pt, res0, xs, rest, xa, rest0, res1, cs, cr, part, rs, rr,
    load, load_st, load_w, load_o, load_x, load_r, a_s, a_r, w_s, w_r, o_s, o_r,
    b_s, b_r, q_s, q_r, c_s, c_r, r_s, r_r, t_s, t_r, tf_s, g_s, g_r, h_s, h_r, hf_s, hx_r,
    k_s, k_r, n_s, n_r, e_s, e_r,
):
    t, d = lax.axis_index("tp"), lax.axis_index("dp")
    z, y, x, c = t // 4, t % 4, d // 2, d % 2
    other = 1 - c
    barrier = pltpu.get_barrier_semaphore()
    greeted = [(z, (y + i) % 4, x, c) for i in (1, 2, 3)]
    greeted += [((z + i) % 4, y, x, c) for i in (1, 2, 3)]
    greeted += [(z, y, (x + i) % 4, (c + k) % 2) for i in range(4) for k in range(2) if i + k]
    for peer in greeted:
        pl.semaphore_signal(barrier, inc=1, device_id=device(*peer), device_id_type=MESH)

    tok_load = pltpu.make_async_copy(tok, xg.at[y], load_x.at[0])
    win_loads = [
        pltpu.make_async_copy(win.at[0], wi.at[0], load_w.at[0]),
        pltpu.make_async_copy(win.at[1], wt.at[d], load_w.at[1]),
    ]
    raw_loads = [
        pltpu.make_async_copy(w.at[0, :, pl.ds(i * 128, 128)], w_raw.at[i, k], load_r.at[i * 2 + k])
        for i in range(4) for k, w in enumerate((wv, wg))
    ]
    wo_loads = [
        pltpu.make_async_copy(w.at[1], wo.at[y, k], load_o.at[1, k]) for k, w in enumerate((wv, wg))
    ]
    small = [(decay, decay_v), (freq, freq_v), (step, step_v), (sin, sin_v), (rdo, rdo_v),
             (skip, skip_v)]
    small_loads = [
        pltpu.make_async_copy(src, dst, load.at[i]) for i, (src, dst) in enumerate(small)
    ]
    gain_load = pltpu.make_async_copy(gain, gain_v, load.at[6])
    st_load = pltpu.make_async_copy(st, st_v, load_st.at[0])
    for copy in [win_loads[0], tok_load, gain_load] + raw_loads + [win_loads[1]] + small_loads + [
        st_load
    ] + wo_loads:
        copy.start()

    plane = [(i, k) for i in range(4) for k in range(4) if i + k]
    plane.sort(key=lambda ik: -(min(ik[0], 4 - ik[0]) + min(ik[1], 4 - ik[1])))

    def peer_of(i, k, core):
        return device((z + i) % 4, (y + k) % 4, x, core)

    sends = Sends()
    win_loads[0].wait()
    tok_load.wait()
    gain_load.wait()
    gain_all[d] = gain_v[1:2]
    pl.semaphore_wait(barrier, len(greeted))

    for i in (2, 1, 3):
        sends.go(wi.at[0], wi.at[i], w_s.at[i], w_r.at[i], device((z + i) % 4, y, x, c))
    for i in (2, 1, 3):
        sends.go(xg.at[y], xg.at[y], a_s.at[i], a_r.at[y], device(z, (y + i) % 4, x, c))
    for copy in raw_loads:
        copy.wait()
    for i in (2, 1, 3):
        yy = (y + i) % 4
        sends.go(w_raw.at[yy], wy.at[y], h_s.at[i], h_r.at[y], device(z, yy, x, c))
    win_loads[1].wait()
    for i in (2, 1, 3):
        sends.go(wt.at[d], wt.at[d], t_s.at[i], t_r.at[d], device(z, y, (x + i) % 4, c))
    for i in (2, 1, 3, 0):
        for k in range(2):
            if i + k:
                sends.go(gain_all.at[d], gain_all.at[d], g_s.at[i * 2 + k], g_r.at[d],
                         device(z, y, (x + i) % 4, (c + k) % 2))

    def send_wo(k):
        wo_loads[k].wait()
        for i in (2, 1, 3):
            sends.go(wo.at[y, k], wo.at[y, k], o_s.at[k, i], o_r.at[k, y],
                     device(z, (y + i) % 4, x, c))

    for copy in small_loads:
        copy.wait()
    rate = jnp.concatenate([decay_v[0], decay_v[1]], axis=0)
    often = jnp.concatenate([freq_v[0], freq_v[1]], axis=0)
    steps = step_v[...]
    times = jnp.concatenate(
        [jnp.broadcast_to(steps[l:l + 1, g:g + 1], (1, 64)) for l in range(L) for g in range(4)],
        axis=0,
    )
    magnitude = jnp.exp(-rate * times)
    angle = often * times
    keep_r = magnitude * jnp.cos(angle)
    keep_i = magnitude * jnp.sin(angle)
    minus = keep_r - 1.0
    below = rate * rate + often * often
    lift_r = (-minus * rate + keep_i * often) / below
    lift_i = (-keep_i * rate - minus * often) / below
    keep_r = jnp.concatenate([keep_r, keep_r], axis=1)
    keep_i = jnp.concatenate([-keep_i, keep_i], axis=1)
    lift_r = jnp.concatenate([lift_r, lift_r], axis=1)
    lift_i = jnp.concatenate([-lift_i, lift_i], axis=1)

    rows = lax.broadcasted_iota(jnp.int32, (128, 128), 0)
    lanes = lax.broadcasted_iota(jnp.int32, (128, 128), 1)
    same_group = rows // 16 == lanes // 16
    lane16 = lax.broadcasted_iota(jnp.int32, (16, 128), 1)
    row16 = lax.broadcasted_iota(jnp.int32, (16, 128), 0)
    low = lane16 < 64

    st_load.wait()

    def prepare(l):
        lifted = []
        for g in range(4):
            k = l * 4 + g
            b = sin_v[l, g]
            lifted.append(lift_r[k:k + 1] * b + lift_i[k:k + 1] * pltpu.roll(b, 64, 1))
        both = jnp.concatenate(lifted + lifted, axis=0)
        big_b[l] = both
        out = jnp.concatenate([rdo_v[l, g] for g in range(4)] * 2, axis=0)
        skips = jnp.concatenate([skip_v[l:l + 1], skip_v[l:l + 1]], axis=1)
        m = jnp.where(same_group, nt(both, out, HIGH), 0.0)
        m = m + jnp.where(rows == lanes, jnp.broadcast_to(skips, (128, 128)), 0.0)
        hi = m.astype(BF16)
        m3[l] = jnp.concatenate([hi, hi, (m - hi.astype(F32)).astype(BF16)], axis=0)
        for g in range(4):
            k = l * 4 + g
            s = st_v[l, :, g, :]
            kept = keep_r[k:k + 1] * s + keep_i[k:k + 1] * pltpu.roll(s, 64, 1)
            ks[l, g * 2] = kept[:16]
            ks[l, g * 2 + 1] = kept[16:]
        prod = nt(ks[l].reshape(128, 128), out, HIGH)
        total = jnp.zeros((16, 128), F32)
        for g in range(4):
            for h in range(2):
                block = prod[(g * 2 + h) * 16:(g * 2 + h) * 16 + 16]
                total = total + jnp.where(lane16 // 16 == h * 4 + g, block, 0.0)
        base[l] = total

    prepare(0)
    prepare(1)

    def read_out(l, raw, scale):
        hi = raw.astype(BF16)
        lo = (raw - hi.astype(F32)).astype(BF16)
        mixed = jnp.dot(
            jnp.concatenate([hi, lo, hi], axis=1), m3[l], preferred_element_type=F32
        )
        return jax.nn.gelu(base[l] + scale * mixed)

    def new_states(l, drive):
        pieces = [
            jnp.where(lane16 // 16 == h * 4 + g, drive, 0.0) for g in range(4) for h in range(2)
        ]
        push = jnp.dot(
            jnp.concatenate(pieces, axis=0), big_b[l], precision=HIGH, preferred_element_type=F32
        )
        for g in range(4):
            for h in range(2):
                k = g * 2 + h
                st_out[l, h * 16:h * 16 + 16, g, :] = ks[l, k] + push[k * 16:k * 16 + 16]

    lane = lax.broadcasted_iota(jnp.int32, (1, 128), 1) // 32

    def regroup(tiles, first_block, mine):
        out = None
        for a, tile in enumerate(tiles):
            piece = pltpu.roll(tile, 32 * ((mine(a) - first_block(a)) % 4), 1)
            out = piece if out is None else jnp.where(lane == mine(a), piece, out)
        return out

    for k in range(4):
        @pl.when(y != k)
        def _(k=k):
            arrived(xg.at[k], a_r.at[k])
    wide = xg[...].reshape(64, 512).astype(F32)
    gained = (wide * gain_v[0:1]).astype(BF16)
    square = jnp.sum(wide * wide, axis=1, keepdims=True)
    row32 = lax.broadcasted_iota(jnp.int32, (32, 128), 0)
    lane32 = lax.broadcasted_iota(jnp.int32, (32, 128), 1)
    for k in range(2):
        part_sq = jnp.where(row32 == lane32, square[k * 32:k * 32 + 32], 0.0)
        sq[k] = jnp.sum(part_sq, axis=0, keepdims=True)

    def project(i):
        if i:
            arrived(wi.at[i], w_r.at[i])
        prod = nt(gained, jnp.concatenate([wi[i], wi[i]], axis=0))
        for k in range(2):
            upper = prod[k * 32:k * 32 + 16]
            lower = prod[k * 32 + 16:k * 32 + 32]
            pb[i, k] = jnp.where(low, upper, lower).astype(BF16)
        for k in range(2):
            to = device((z - i) % 4, y, z, k)
            here = None if i else (x == z) & (c == k)
            sends.go(pb.at[i, k], bm.at[d], b_s.at[i * 2 + k], b_r.at[d], to, here)
            sends.go(sq.at[k], bq.at[d], q_s.at[i * 2 + k], q_r.at[d], to, here)

    project(0)

    wy[y] = w_raw[y]
    for k in range(4):
        @pl.when(y != k)
        def _(k=k):
            arrived(wy.at[k], h_r.at[k])
        turned = jnp.transpose(wy[k].reshape(128, 128).astype(F32)).astype(BF16)
        for i in range(4):
            wz[i, k] = turned[i * 32:i * 32 + 32]
    for i in (2, 1, 3):
        zz = (z + i) % 4
        sends.go(wz.at[zz], w0.at[x, z], h_s.at[4 + i], h_r.at[4 + z], device(zz, y, x, c))
    w0[x, z] = wz[z]

    def replicate(i):
        zz = (z + i) % 4
        if i:
            arrived(w0.at[x, zz], h_r.at[4 + zz])
        for k in (2, 1, 3):
            sends.go(w0.at[x, zz], w0.at[x, zz], hf_s.at[i, k], hx_r.at[x, zz],
                     device(z, y, (x + k) % 4, c))

    send_wo(0)
    send_wo(1)

    for i in (1, 3, 2):
        project(i)
    for i in range(4):
        k = ((x + i) % 4) * 2 + c
        if i:
            arrived(wt.at[k], t_r.at[k])
        sends.go(wt.at[k], wt.at[k], tf_s.at[i], t_r.at[k], device(z, y, x, other))

    for i in (0, 1, 3, 2):
        replicate(i)
    mine = pl.ds(pl.multiple_of(y * 128, 128), 128)
    blocks = [xg[a, :, mine].astype(F32) for a in range(4)]
    for i in range(4):
        zz = (z - i) % 4
        pt[i] = regroup(blocks, lambda a: zz, lambda a: a).astype(BF16)
        here = None if i else x == z
        sends.go(pt.at[i], res0.at[x], e_s.at[i], e_r.at[x], device(zz, y, z, c), here)

    for k in range(8):
        arrived(bq.at[k], q_r.at[k])
        arrived(bm.at[k], b_r.at[k])
    squares = bq[0]
    raw = bm[0].astype(F32)
    for k in range(1, 8):
        squares = squares + bq[k]
        raw = raw + bm[k].astype(F32)
    spread = jnp.broadcast_to(squares, (16, 128))
    first = jnp.sum(jnp.where(lane16 == row16, spread, 0.0), axis=1, keepdims=True)
    second = jnp.sum(jnp.where(lane16 == row16 + 16, spread, 0.0), axis=1, keepdims=True)
    scale = lax.rsqrt(jnp.where(low, first, second) * (1.0 / D) + EPS)
    side = y % 2
    ready = read_out(0, raw, scale)
    rg[c, t] = ready.astype(BF16)
    for i, k in plane + [(0, 0)]:
        for n, core in enumerate((c, other)):
            if i + k + n:
                sends.go(rg.at[c, t], rg.at[c, t], k_s.at[n, i * 4 + k], k_r.at[c, t],
                         peer_of(i, k, core))

    new_states(0, scale * raw)

    for i in range(4):
        arrived(wt.at[2 * i + other], t_r.at[2 * i + other])
    for k in range(8):
        @pl.when(d != k)
        def _(k=k):
            arrived(gain_all.at[k], g_r.at[k])
    for k in range(16):
        tile = slice((k % 4) * 128, (k % 4) * 128 + 128)
        for g in range(2):
            wp[k, g] = regroup(
                [wt[2 * a + g, :, tile].astype(F32) for a in range(4)], lambda a: k // 4, lambda a: a
            ).astype(BF16)
            gain_p[k, g] = regroup(
                [gain_all[2 * a + g, :, tile] for a in range(4)], lambda a: k // 4, lambda a: a
            )

    for a in range(4):
        arrived(res0.at[a], e_r.at[a])
    for k in range(4):
        rest0[k] = regroup(
            [res0[a].astype(F32) for a in range(4)], lambda a: k, lambda a: a
        )

    near_first = [(0, 0)] + plane[::-1]
    for i, k in near_first:
        s = ((z + i) % 4) * 4 + (y + k) % 4
        for n, core in enumerate((c, other)):
            if i + k + n:
                arrived(rg.at[core, s], k_r.at[core, s])
    chunks = []
    for k in range(16):
        tops, bottoms = [], []
        for n in range(2):
            own = rg[n, k].astype(F32)
            swapped = pltpu.roll(own, 64, 1)
            tops += [jnp.where(low, own, 0.0), jnp.where(low, swapped, 0.0)]
            bottoms += [jnp.where(low, 0.0, swapped), jnp.where(low, 0.0, own)]
        chunks.append(jnp.concatenate(tops + bottoms, axis=0).astype(BF16))
    for i in (1, 3, 2):
        for k in range(4):
            arrived(w0.at[(x + i) % 4, k], hx_r.at[(x + i) % 4, k])
    both = jnp.zeros((128, 128), F32)
    for j in range(0, 16, 2):
        right = [w0[:, k // 4, k % 4].reshape(128, 128) for k in (j, j + 1)]
        left = jnp.concatenate(chunks[j:j + 2], axis=1)
        both = both + nt(left, jnp.concatenate(right, axis=1))
    current = rest0[...].reshape(64, 128) + both[:64] * jax.nn.sigmoid(both[64:])
    xs[0] = current[:32].astype(BF16)
    xs[1] = current[32:].astype(BF16)
    for i, k in plane + [(0, 0)]:
        for n, core in enumerate((c, other)):
            if i + k + n:
                sends.go(xs.at[core], xa.at[t, c], n_s.at[n, i * 4 + k], n_r.at[c, t],
                         peer_of(i, k, core))
    xa[t, c] = xs[c]

    total = jnp.zeros((32, 128), F32)
    square = jnp.zeros((32, 128), F32)
    for i, k in near_first:
        s = ((z + i) % 4) * 4 + (y + k) % 4
        for n, core in enumerate((c, other)):
            if i + k + n:
                arrived(xa.at[s, core], n_r.at[core, s])
        gained = []
        for n in range(2):
            wide = xa[s, n].astype(F32)
            square = square + wide * wide
            gained.append((wide * gain_p[s, n]).astype(BF16))
        right = jnp.concatenate([wp[s, 0], wp[s, 1]], axis=1)
        right = jnp.concatenate([right, right], axis=0)
        total = total + nt(jnp.concatenate(gained, axis=1), right)
    square = jnp.sum(square, axis=1, keepdims=True)
    raw = jnp.where(low, total[:16], total[16:])
    scale = lax.rsqrt(jnp.where(low, square[:16], square[16:]) * (1.0 / D) + EPS)
    ready = read_out(1, raw, scale)
    turned = pltpu.roll(ready, 64, 1)
    for h in range(2):
        placed = jnp.where(side == h, ready, turned)
        cs[h] = jnp.where(lane16 // 64 == side, placed, 0.0).astype(BF16)
    for h in range(2):
        yy = 2 * c + h
        for i in (2, 1, 3, 0):
            for k in range(2):
                here = y == yy if i + k == 0 else None
                sends.go(cs.at[h], cr.at[x, y], c_s.at[h * 8 + i * 2 + k],
                         c_r.at[x, y], device(z, yy, (x + i) % 4, (c + k) % 2), here)
    new_states(1, scale * raw)

    half_to, d_to = z // 2, t % 8
    for k in range(4):
        tiles = []
        for i in range(4):
            tiles.append(
                xa[i * 4 + k, d_to % 2, pl.ds(pl.multiple_of(half_to * 16, 16), 16), :].astype(F32)
            )
        rest[:, k * 128:k * 128 + 128] = regroup(tiles, lambda a: d_to // 2, lambda a: a).astype(BF16)
    here = (z == x) & (y == 2 * c + half_to) & (d == d_to)
    sends.go(rest, res1, e_s.at[8], e_r.at[8],
             device(x, 2 * c + half_to, d_to // 2, d_to % 2), here)

    for k in range(4):
        @pl.when(y != k)
        def _(k=k):
            for i in range(2):
                arrived(wo.at[k, i], o_r.at[i, k])
    for i in range(4):
        for k in range(4):
            arrived(cr.at[i, k], c_r.at[i, k])
    left = jnp.concatenate(
        [(cr[:, 2 * j] + cr[:, 2 * j + 1]).reshape(64, 128) for j in range(2)], axis=1
    )
    for k in range(2):
        prod = jnp.dot(left, wo[:, k].reshape(256, 512), preferred_element_type=F32)
        for i in range(4):
            part[i, k] = prod[i * 16:i * 16 + 16]
            rs[i, k] = prod[i * 16:i * 16 + 16].astype(BF16)
        for i in (2, 1, 3):
            zz = (z + i) % 4
            sends.go(rs.at[zz, k], rr.at[i, k], r_s.at[k, i], r_r.at[k, i], device(zz, y, x, c))
    sends.finish(6)
    value, gate = part[z, 0], part[z, 1]
    for i in (1, 3, 2):
        for k in range(2):
            arrived(rr.at[i, k], r_r.at[k, i])
        value = value + rr[i, 0].astype(F32)
        gate = gate + rr[i, 1].astype(F32)
    arrived(res1, e_r.at[8])
    before = res1[...].astype(F32)
    tok_out[...] = (before + value * jax.nn.sigmoid(gate)).astype(BF16)
    sends.finish()


def layers(*args):
    args = list(args)
    args[2] = jnp.swapaxes(args[2], 1, 2)
    dma = pltpu.SemaphoreType.DMA
    v = pltpu.VMEM
    anywhere = pl.BlockSpec(memory_space=pl.ANY)
    scratch = [
        v((4, 16, 512), BF16),
        v((4, 64, 512), BF16),
        v((8, 64, 512), BF16),
        v((4, 2, 64, 128), BF16),
        v((4, 2, 64, 128), BF16),
        v((4, 4, 32, 128), BF16),
        v((4, 4, 4, 32, 128), BF16),
        v((16, 2, 64, 128), BF16),
        v((16, 2, 1, 128), F32),
        v((4, 2, 64, 512), BF16),
        v((L, 512), F32),
        v((8, 1, 512), F32),
        v((L, 4, 64), F32),
        v((L, 4, 64), F32),
        v((L, 4), F32),
        v((L, 4, 16, 128), F32),
        v((L, 4, 16, 128), F32),
        v((L, 64), F32),
        v((L, 32, 4, 128), F32),
        v((L, 128, 128), F32),
        v((L, 384, 128), BF16),
        v((L, 16, 128), F32),
        v((L, 8, 16, 128), F32),
        v((4, 2, 16, 128), BF16),
        v((2, 1, 128), F32),
        v((8, 16, 128), BF16),
        v((8, 1, 128), F32),
        v((2, 16, 16, 128), BF16),
        v((4, 16, 128), BF16),
        v((4, 16, 128), BF16),
        v((2, 32, 128), BF16),
        v((16, 512), BF16),
        v((16, 2, 32, 128), BF16),
        v((4, 16, 128), F32),
        v((16, 512), BF16),
        v((2, 16, 128), BF16),
        v((4, 4, 16, 128), BF16),
        v((4, 2, 16, 512), F32),
        v((4, 2, 16, 512), BF16),
        v((4, 2, 16, 512), BF16),
        dma((7,)), dma((1,)), dma((2,)), dma((2, 2)), dma((1,)), dma((8,)),
        dma((4,)), dma((4,)),
        dma((4,)), dma((4,)),
        dma((2, 4)), dma((2, 4)),
        dma((8,)), dma((8,)),
        dma((8,)), dma((8,)),
        dma((16,)), dma((4, 4)),
        dma((2, 4)), dma((2, 4)),
        dma((4,)), dma((8,)), dma((4,)),
        dma((8,)), dma((8,)),
        dma((8,)), dma((8,)), dma((4, 4)),
        dma((4, 4)),
        dma((2, 16)), dma((2, 16)),
        dma((2, 16)), dma((2, 16)),
        dma((9,)), dma((9,)),
    ]
    return pl.pallas_call(
        kernel,
        out_shape=(
            pltpu.VMEM((16, 512), BF16),
            pltpu.VMEM((L, 32, 4, 128), F32),
        ),
        in_specs=[anywhere] * 12,
        out_specs=(pl.BlockSpec(memory_space=pltpu.VMEM),)*2,
        scratch_shapes=scratch,
        compiler_params=pltpu.CompilerParams(collective_id=0, has_side_effects=True),
        name="layers",
    )(*args)


def tail(new_tokens, new_states, tokens_out, states_out, sem):
    copies = [
        pltpu.make_async_copy(new_states, states_out, sem.at[0]),
        pltpu.make_async_copy(new_tokens, tokens_out, sem.at[1]),
    ]
    for copy in copies:
        copy.start()
    for copy in copies:
        copy.wait()


def body(*args):
    vmem = pl.BlockSpec(memory_space=pltpu.VMEM)
    anywhere = pl.BlockSpec(memory_space=pl.ANY)
    results = [pltpu.with_memory_space_constraint(a, pltpu.VMEM) for a in layers(*args)]
    return pl.pallas_call(
        tail,
        out_shape=tuple(jax.ShapeDtypeStruct(a.shape, a.dtype) for a in results),
        in_specs=[vmem] * 2,
        out_specs=(anywhere, anywhere),
        scratch_shapes=[pltpu.SemaphoreType.DMA((2,))],
        name="tail",
    )(*results)


def solution(mesh):
    in_specs = (
        P("tp", "dp"),
        P(None, "dp"),
        P(None, "dp", "tp"),
        P(None, "tp", None),
        P(None, "tp", None),
        P(None, "tp"),
        P(None, "tp", None, None),
        P(None, "tp", None, None),
        P(None, "tp"),
        P(None, "tp", "dp"),
        P(None, "tp", "dp"),
        P(None, "dp", "tp", None),
    )
    out_specs = (P("tp", "dp"), P(None, "dp", "tp", None))
    return jax.shard_map(body, mesh=mesh, in_specs=in_specs, out_specs=out_specs, check_vma=False)
```
